32 devices in a mesh: grp: 2 (over y), fs: 4 (over z), tp: 4 (over x, core).
Axes of the slice: x: 2, y: 2, z: 4, core: 2. Of those that a mesh axis runs over, the one named last changes fastest.
Arguments:
- tokens: bfloat16 [8192, 2048], P(('grp', 'fs'), 'tp'), parts along dimension 0, may hold values from -50 to 50
- mix_gain: float32 [2048], replicated, may hold values from 0.1 to 1.9
- value_proj: bfloat16 [2048, 1024], P('fs', 'tp'), may hold values from -0.125 to 0.125
- gate_proj: bfloat16 [2048, 1024], P('fs', 'tp'), may hold values from -0.125 to 0.125
- conv_taps: float32 [31, 1024], P(None, 'tp'), may hold values from -1 to 1
- chan_gain: float32 [1024], replicated, may hold values from 0.1 to 1.9
- chan_shift: float32 [1024], replicated, may hold values from -3 to 3
- mix_out: bfloat16 [1024, 2048], P('fs', 'tp'), may hold values from -0.1875 to 0.1875
- mlp_gain: float32 [2048], replicated, may hold values from 0.1 to 1.9
- mlp_gate: bfloat16 [2048, 5632], P('fs', 'tp'), may hold values from -0.125 to 0.125
- mlp_up: bfloat16 [2048, 5632], P('fs', 'tp'), may hold values from -0.125 to 0.125
- gate_taps: float32 [3, 5632], P(None, 'tp'), may hold values from -3.5 to 3.5
- up_taps: float32 [3, 5632], P(None, 'tp'), may hold values from -3.5 to 3.5
- mlp_down: bfloat16 [5632, 2048], P('tp', 'fs'), may hold values from -0.078125 to 0.078125
- final_gain: float32 [2048], P('tp'), may hold values from 0.1 to 1.9
Outputs:
- layer_out: bfloat16 [8192, 2048], P(('grp', 'fs'), 'tp'), parts along dimension 0
The draws below stay inside these ranges and needn't reach their ends.
There are 2 independent parts, one for each index of `grp`. The reference program is written for one: setup_inputs(seed, part) draws one part's arguments, and reference() takes and returns one part's arrays. A program takes and returns all parts, laid end to end along the dimension named above; an argument that names none is the same for every part. Nothing has to cross between parts.
All inputs are finite; a program needn't handle non-finite values.
Results may differ from the reference program's by a relative error of at most 0.0095.
Values may be sent and summed in bfloat16 or wider, within the bound.
A program may use at most 128 MiB of HBM per device.

```python
import math
import jax
import jax.numpy as jnp
from jax import lax

D = 2048
CA = 1024
FF = 5632
KW = 31
FKW = 3
TOK_DEV = 1024
TOKENS = 4096
FF_BLOCK = 1408
N_TP = 4


def draw_tokens(key, part):
    base_key = jax.random.fold_in(key, 7)
    key_rows, key_cols, key_vals = jax.random.split(base_key, 3)
    lowest = 0.3
    values = jnp.clip(jax.random.normal(key_vals, (TOKENS, D), jnp.float32), -4.0, 4.0)
    row_scale = jnp.exp(jax.random.uniform(key_rows, (TOKENS, 1), jnp.float32, math.log(lowest), math.log(3.0)))
    ramp = jnp.exp(jnp.linspace(math.log(0.4), math.log(2.5), D, dtype=jnp.float32))[None, :]
    col_scale = ramp * jnp.exp(jax.random.uniform(key_cols, (1, D), jnp.float32, -0.5, 0.5))
    return (values * row_scale * col_scale).astype(jnp.bfloat16)


def steps_of(key, dims, pieces, least, largest):
    level = 1.0
    for dim, blocks in pieces:
        draws = jax.random.uniform(jax.random.fold_in(jax.random.fold_in(key, 6), dim), (blocks,), jnp.float32, least / len(pieces), largest / len(pieces))
        level = level * jnp.repeat(jnp.exp(draws), dims[dim] // blocks).reshape((-1,) + (1,) * (len(dims) - 1 - dim))
    return level


def normal_values(own_key, extent, scale, reach, cuts=(), kind=jnp.bfloat16):
    array = scale * jax.random.normal(own_key, extent, jnp.float32)
    if cuts:
        array = array * steps_of(own_key, extent, cuts, -0.22, 0.18)
    return jnp.clip(array, -reach, reach).astype(kind)


def setup_inputs(seed: int = 0, part: int = 0) -> dict:
    splits = jax.random.split(jax.random.key(seed), 16)
    part_keys = jax.random.split(jax.random.fold_in(splits[15], part), 16)
    return {
        "tokens": draw_tokens(jax.random.fold_in(jax.random.fold_in(splits[15], part), 71), part),
        "mix_gain": jnp.clip(1.0 + 0.18 * jax.random.normal(splits[1], (D,), jnp.float32), 0.1, 1.9),
        "value_proj": normal_values(splits[2], (D, CA), D ** -0.5, 0.125, ((0, 4), (1, 4))),
        "gate_proj": normal_values(splits[3], (D, CA), D ** -0.5, 0.125, ((0, 4), (1, 4))),
        "conv_taps": normal_values(splits[4], (KW, CA), KW ** -0.5, 1.0, ((1, 4),), jnp.float32),
        "chan_gain": jnp.clip(1.0 + 0.18 * jax.random.normal(splits[5], (CA,), jnp.float32), 0.1, 1.9),
        "chan_shift": normal_values(splits[6], (CA,), 0.5, 3.0, (), jnp.float32),
        "mix_out": normal_values(splits[7], (CA, D), CA ** -0.5, 0.1875, ((0, 4), (1, 4))),
        "mlp_gain": jnp.clip(1.0 + 0.18 * jax.random.normal(splits[8], (D,), jnp.float32), 0.1, 1.9),
        "mlp_gate": normal_values(splits[9], (D, FF), D ** -0.5, 0.125, ((0, 4), (1, 4))),
        "mlp_up": normal_values(splits[10], (D, FF), D ** -0.5, 0.125, ((0, 4), (1, 4))),
        "gate_taps": normal_values(splits[11], (FKW, FF), FKW ** -0.5, 3.5, ((1, 4),), jnp.float32),
        "up_taps": normal_values(splits[12], (FKW, FF), FKW ** -0.5, 3.5, ((1, 4),), jnp.float32),
        "mlp_down": normal_values(splits[13], (FF, D), FF ** -0.5, 0.078125, ((0, 4), (1, 4))),
        "final_gain": jnp.clip(1.0 + 0.18 * jax.random.normal(splits[14], (D,), jnp.float32), 0.1, 1.9),
    }


def rms_scale(values, gain):
    return values * lax.rsqrt(lax.optimization_barrier(jnp.mean(values * values, axis=-1, keepdims=True)) + 1e-06) * gain

def along_sequences(values, taps, seq_len):
    width = taps.shape[0]
    half = (width - 1) // 2
    channels = values.shape[1]
    grouped = values.reshape(-1, seq_len, channels)
    padded = jnp.pad(grouped, ((0, 0), (half, width - 1 - half), (0, 0)))
    total = jnp.zeros_like(grouped)
    for offset in range(width):
        total = total + taps[offset] * padded[:, offset:offset + seq_len]
    return total.reshape(values.shape)

def reference(tokens, mix_gain, value_proj, gate_proj, conv_taps, chan_gain, chan_shift, mix_out, mlp_gain, mlp_gate, mlp_up, gate_taps, up_taps, mlp_down, final_gain):
    base = tokens.astype(jnp.float32)
    normed = rms_scale(base, mix_gain).astype(jnp.bfloat16)
    value = jnp.dot(normed, value_proj, preferred_element_type=jnp.float32)
    gate = jnp.dot(normed, gate_proj, preferred_element_type=jnp.float32)
    glu = value * jax.nn.sigmoid(gate)
    conv_out = along_sequences(glu, conv_taps, TOK_DEV).astype(jnp.bfloat16)
    conv_wide = conv_out.astype(jnp.float32)
    mean = lax.optimization_barrier(jnp.mean(conv_wide, axis=-1, keepdims=True))
    var = lax.optimization_barrier(jnp.mean(conv_wide * conv_wide, axis=-1, keepdims=True)) - mean * mean
    chan_norm = (conv_wide - mean) * lax.rsqrt(var + 1e-05) * chan_gain + chan_shift
    hidden_mix = jax.nn.silu(chan_norm).astype(jnp.bfloat16)
    mixed = (base + jnp.dot(hidden_mix, mix_out, preferred_element_type=jnp.float32)).astype(jnp.bfloat16)
    mixed_wide = mixed.astype(jnp.float32)
    normed_two = rms_scale(mixed_wide, mlp_gain).astype(jnp.bfloat16)
    gate_conv = along_sequences(jnp.dot(normed_two, mlp_gate, preferred_element_type=jnp.float32), gate_taps, TOK_DEV)
    up_conv = along_sequences(jnp.dot(normed_two, mlp_up, preferred_element_type=jnp.float32), up_taps, TOK_DEV)
    hidden_mlp = (jax.nn.silu(gate_conv) * up_conv).astype(jnp.bfloat16)
    mlp_out = jnp.zeros((tokens.shape[0], D), jnp.float32)
    for block in range(N_TP):
        lower = block * FF_BLOCK
        partial_sum = jnp.dot(hidden_mlp[:, lower:lower + FF_BLOCK], mlp_down[lower:lower + FF_BLOCK], preferred_element_type=jnp.float32)
        rounded = lax.optimization_barrier(partial_sum.astype(jnp.bfloat16))
        mlp_out = mlp_out + rounded.astype(jnp.float32)
    summed = mixed_wide + mlp_out
    return rms_scale(summed, final_gain).astype(jnp.bfloat16)
```

```python
import functools
from types import SimpleNamespace

import jax
import jax.numpy as jnp
from jax import lax
from jax.experimental import pallas as pl
from jax.experimental.pallas import tpu as pltpu
from jax.sharding import PartitionSpec as P

MESH = pl.DeviceIdType.MESH
F32, BF16 = jnp.float32, jnp.bfloat16
LANES = 128
CORES = 2
LEAD = 2
PAD = 16
EDGE = 8
BUDGET = 4.5


def column_chunks(width, most):
    return [(first, min(most, width - first)) for first in range(0, width, most)]


def sigmoid(value):
    return 1.0 / (1.0 + jnp.exp(-value))


def layer_kernel(n, *refs):
    arrays = SimpleNamespace(**dict(zip(n.inputs, refs)))
    out = refs[len(n.inputs)]
    s = SimpleNamespace(**dict(zip(n.scratch, refs[len(n.inputs) + 1 :])))

    group, fs, tp = lax.axis_index("grp"), lax.axis_index("fs"), lax.axis_index("tp")
    chip, core = tp // CORES, tp % CORES
    sibling = tp + 1 - 2 * core

    def chip_at(jump):
        return (chip + jump + n.chips) % n.chips

    def rows_of(r):
        return pl.ds(r * n.rows, n.rows)

    local = {}

    def load(name, src, dst):
        index = len(local)
        local[name] = pltpu.make_async_copy(src, dst, s.local_sem.at[index])
        local[name].start()

    loaded = set()

    def have(*names):
        for name in names:
            if name not in loaded:
                loaded.add(name)
                local[name].wait()

    def own_rows(dst, count):
        return dst.at[pl.ds(pl.multiple_of(fs * count, count), count), :]

    load("tokens", arrays.tokens, s.tok.at[tp])
    for name in n.small:
        load(name, getattr(arrays, name), getattr(s, "v_" + name))
    load("value", arrays.value, own_rows(s.wv, n.depth))
    load("gate", arrays.gate, own_rows(s.wg, n.depth))
    load("mix", arrays.mix, own_rows(s.wm, n.mix_depth))
    load("mgate", arrays.mgate, own_rows(s.wgate, n.depth))
    load("mup", arrays.mup, own_rows(s.wup, n.depth))
    load("down", arrays.down, s.wd.at[fs])

    chunks = [
        (arrays.value, s.wv, n.depth, 0, n.own_channels),
        (arrays.gate, s.wg, n.depth, 0, n.own_channels),
        (arrays.mix, s.wm, n.mix_depth, 0, n.cols),
    ]
    first_mlp = len(chunks)
    for first, width in n.mlp_cols:
        chunks.append((arrays.mgate, s.wgate, n.depth, first, width))
        chunks.append((arrays.mup, s.wup, n.depth, first, width))
    first_down = len(chunks)
    for j in range(n.down_blocks):
        chunks.append((arrays.down, s.wd, n.hidden, j * LANES, LANES))
    assert len(chunks) == n.chunks

    def slot(i, f, part):
        _, dst, depth, first, width = chunks[i]
        half = depth // n.groups
        columns = pl.ds(first, width)
        if i >= first_down:
            return dst.at[f, pl.ds(pl.multiple_of(part * half, half), half), columns]
        return dst.at[pl.ds(pl.multiple_of(f * depth + part * half, half), half), columns]

    def z_copy(i, f, to, sems, own=False):
        src = slot(i, f, group)
        if own:
            source, _, depth, first, width = chunks[i]
            half = depth // n.groups
            src = source.at[pl.ds(pl.multiple_of(group * half, half), half), pl.ds(first, width)]
        return pltpu.make_async_remote_copy(
            src_ref=src,
            dst_ref=slot(i, f, group),
            send_sem=sems.at[i, f],
            recv_sem=s.z_recv.at[i, f],
            device_id={"fs": to},
            device_id_type=MESH,
        )

    def y_copy(i, f, jump, part):
        return pltpu.make_async_remote_copy(
            src_ref=slot(i, f, part),
            dst_ref=slot(i, f, part),
            send_sem=s.y_send.at[jump - 1, i, f],
            recv_sem=s.y_recv.at[jump - 1, i, f],
            device_id={"grp": (group + jump) % n.groups},
            device_id_type=MESH,
        )

    last = n.shards - 1
    reach = jnp.minimum(fs, last - fs)

    def arrival(step):
        near = fs - (step + 1) // 2 if step % 2 else fs + (step + 1) // 2
        distance = step - reach
        far = jnp.where(fs > last - fs, fs - distance, fs + distance)
        return jnp.where(step <= 2 * reach, near, far)

    def send_own(i):
        @pl.when(fs < last)
        def _():
            z_copy(i, fs, fs + 1, s.up_send, own=True).start()

        @pl.when(fs > 0)
        def _():
            z_copy(i, fs, fs - 1, s.down_send, own=True).start()

    def pump(i, step):
        f = arrival(step)
        z_copy(i, f, fs, s.up_send).wait_recv()

        @pl.when(jnp.logical_and(f < fs, fs < last))
        def _():
            z_copy(i, f, fs + 1, s.up_send).start()

        @pl.when(jnp.logical_and(f > fs, fs > 0))
        def _():
            z_copy(i, f, fs - 1, s.down_send).start()

        for jump in range(1, n.groups):
            y_copy(i, f, jump, group).start()

    def wait_y(i, f):
        for jump in range(1, n.groups):
            y_copy(i, f, jump, (group - jump + n.groups) % n.groups).wait_recv()

    def ready(i):
        for step in range(1, n.shards):
            wait_y(i, arrival(step))

    def drain_chunk(i):
        @pl.when(fs < last)
        def _():
            z_copy(i, fs, fs + 1, s.up_send, own=True).wait_send()

        @pl.when(fs > 0)
        def _():
            z_copy(i, fs, fs - 1, s.down_send, own=True).wait_send()

        for step in range(1, n.shards):
            f = arrival(step)

            @pl.when(jnp.logical_and(f < fs, fs < last))
            def _():
                z_copy(i, f, fs + 1, s.up_send).wait_send()

            @pl.when(jnp.logical_and(f > fs, fs > 0))
            def _():
                z_copy(i, f, fs - 1, s.down_send).wait_send()

            for jump in range(1, n.groups):
                y_copy(i, f, jump, group).wait_send()

    class Gather:
        def __init__(self, blocks, kind, own=None):
            self.blocks, self.kind, self.own = blocks, kind, own

        def copy(self, block, r, to, send, src=None):
            dst = self.blocks.at[block, rows_of(r), :]
            return pltpu.make_async_remote_copy(
                src_ref=dst if src is None else src,
                dst_ref=dst,
                send_sem=s.gather_send.at[self.kind, send, r],
                recv_sem=s.gather_recv.at[self.kind, block, r],
                device_id={"tp": to},
                device_id_type=MESH,
            )

        def own_copies(self, r):
            src = None if self.own is None else self.own.at[rows_of(r), :]
            copies = [
                self.copy(tp, r, chip_at(jump) * CORES + core, jump, src)
                for jump in range(1, n.chips)
            ]
            return copies + [self.copy(tp, r, sibling, 0, src)]

        def passed(self, r, jump):
            block = chip_at(-jump) * CORES + core
            return self.copy(block, r, sibling, n.chips - 1 + jump)

        def send(self, r):
            for copy in self.own_copies(r):
                copy.start()

        def forward(self, r):
            for jump in range(1, n.chips):
                copy = self.passed(r, jump)
                copy.wait_recv()
                copy.start()

        def wait(self, r):
            self.copy(sibling, r, sibling, 0).wait_recv()
            for jump in range(1, n.chips):
                block = chip_at(-jump) * CORES + 1 - core
                self.copy(block, r, sibling, 0).wait_recv()

        def drain(self, r):
            for copy in self.own_copies(r):
                copy.wait_send()
            for jump in range(1, n.chips):
                self.passed(r, jump).wait_send()

    tok = Gather(s.tok, 0, arrays.tokens)
    cv = Gather(s.cv, 1)
    mx = Gather(s.mx, 2)

    def each_tile(r, size, body):
        def step(q, carry):
            body(pl.multiple_of(r * n.rows + q * size, size))
            return carry

        lax.fori_loop(0, n.rows // size, step, 0)

    def norm_rows(blocks, gain, r):
        def body(first):
            rows = pl.ds(first, 32)
            total = jnp.zeros((32, 1), F32)
            for t in range(n.tps):
                v = blocks[t, rows, :].astype(F32)
                total = total + jnp.sum(v * v, axis=-1, keepdims=True)
            scale = lax.rsqrt(total / n.width + 1e-06)
            for t in range(n.tps):
                columns = slice(t * n.cols, (t + 1) * n.cols)
                v = blocks[t, rows, :].astype(F32)
                s.xn[rows, columns] = (v * scale * gain[:, columns]).astype(BF16)

        each_tile(r, 32, body)

    def dot(a, b):
        return jnp.dot(a, b, preferred_element_type=F32)

    def norm_one(r):
        have("tokens", "mix_gain")
        tok.wait(r)
        norm_rows(s.tok, s.v_mix_gain, r)

    def mix_in(r):
        if r == 0:
            have("value", "gate", "conv_taps")
            ready(0)
            ready(1)
        x = s.xn[rows_of(r), :]
        value = dot(x, s.wv[...])
        gate = dot(x, s.wg[...])
        s.glu[pl.ds(PAD + r * n.rows, n.rows), :] = value * sigmoid(gate)

    def conv(r):
        tile, half = 64, (n.taps - 1) // 2
        window = tile + 2 * PAD
        for lanes in range(0, n.own_channels, LANES):
            columns = slice(lanes, lanes + LANES)

            def body(first):
                x = s.glu[pl.ds(first, window), columns]
                total = jnp.zeros((tile, LANES), F32)
                for shift in range(8):
                    moved = pltpu.roll(x, window - shift, 0) if shift else x
                    for k in range(n.taps):
                        at = PAD - half + k
                        if at % 8 == shift:
                            piece = moved[at - shift : at - shift + tile]
                            total = total + s.v_conv_taps[k : k + 1, columns] * piece
                s.cv[tp, pl.ds(first, tile), columns] = total.astype(BF16)

            each_tile(r, tile, body)
        cv.send(r)

    def mix_result(r):
        if r == 0:
            have("chan_gain", "chan_shift", "mix")
            ready(2)
        cv.wait(r)

        def body(first):
            rows = pl.ds(first, 32)
            total = jnp.zeros((32, 1), F32)
            square = jnp.zeros((32, 1), F32)
            for t in range(n.tps):
                v = s.cv[t, rows, :].astype(F32)
                total = total + jnp.sum(v, axis=-1, keepdims=True)
                square = square + jnp.sum(v * v, axis=-1, keepdims=True)
            mean = total / n.channels
            scale = lax.rsqrt(square / n.channels - mean * mean + 1e-05)
            for t in range(n.tps):
                columns = slice(t * n.own_channels, (t + 1) * n.own_channels)
                v = s.cv[t, rows, :].astype(F32)
                v = (v - mean) * scale * s.v_chan_gain[:, columns] + s.v_chan_shift[:, columns]
                s.hm[rows, columns] = (v * sigmoid(v)).astype(BF16)

        each_tile(r, 32, body)
        rows = rows_of(r)
        result = dot(s.hm[rows, :], s.wm[...])
        s.mx[tp, rows, :] = (s.tok[tp, rows, :].astype(F32) + result).astype(BF16)
        mx.send(r)

    def norm_two(r):
        have("mlp_gain")
        mx.wait(r)
        norm_rows(s.mx, s.v_mlp_gain, r)

    def mlp_in(c, r):
        first, width = n.mlp_cols[c]
        if r == 0:
            have("mgate", "mup", "gate_taps", "up_taps")
            ready(first_mlp + 2 * c)
            ready(first_mlp + 2 * c + 1)
        x = s.xn[rows_of(r), :]
        rows = pl.ds(EDGE + r * n.rows, n.rows)
        s.gp[rows, :width] = dot(x, s.wgate[:, first : first + width])
        s.up[rows, :width] = dot(x, s.wup[:, first : first + width])

    def mlp_act(c, r):
        first_column, width = n.mlp_cols[c]
        tile = 32
        window = tile + 2 * EDGE

        def filtered(values, taps, first, lanes, columns):
            x = values[pl.ds(first, window), lanes : lanes + LANES]
            low = pltpu.roll(x, 1, 0)[EDGE : EDGE + tile]
            high = pltpu.roll(x, window - 1, 0)[EDGE : EDGE + tile]
            middle = x[EDGE : EDGE + tile]
            return taps[0:1, columns] * low + taps[1:2, columns] * middle + taps[2:3, columns] * high

        def body(first):
            for lanes in range(0, width, LANES):
                columns = slice(first_column + lanes, first_column + lanes + LANES)
                gate = filtered(s.gp, s.v_gate_taps, first, lanes, columns)
                up = filtered(s.up, s.v_up_taps, first, lanes, columns)
                s.hidden[pl.ds(first, tile), columns] = (gate * sigmoid(gate) * up).astype(BF16)

        each_tile(r, tile, body)

    own_blocks = n.cols // LANES
    pending = []

    def block_of(f, j):
        b = f * n.down_blocks + j
        owner = b // own_blocks
        return b, owner, owner % CORES

    def to_sibling(b):
        return pltpu.make_async_remote_copy(
            src_ref=s.stage.at[b],
            dst_ref=s.sib_in.at[b],
            send_sem=s.stage_send.at[b],
            recv_sem=s.sib_recv.at[b],
            device_id={"tp": sibling},
            device_id_type=MESH,
        )

    def to_owner(b, owner):
        jump = (chip - owner // CORES + n.chips) % n.chips
        index = jnp.maximum(jump - 1, 0)
        return pltpu.make_async_remote_copy(
            src_ref=s.stage.at[b],
            dst_ref=s.own_in.at[index, b % own_blocks],
            send_sem=s.stage_send.at[b],
            recv_sem=s.own_recv.at[index, b % own_blocks],
            device_id={"tp": owner},
            device_id_type=MESH,
        )

    def collect(f, j, keep):
        b, owner, side = block_of(f, j)

        @pl.when(side == core)
        def _():
            to_sibling(b).wait_recv()

            @pl.when(owner == tp)
            def _():
                for r in range(n.pieces):
                    rows = rows_of(r)
                    s.total[b % own_blocks, rows, :] = s.kept[keep, rows, :] + s.sib_in[b, rows, :].astype(F32)

            @pl.when(owner != tp)
            def _():
                for r in range(n.pieces):
                    rows = rows_of(r)
                    both = s.kept[keep, rows, :] + s.sib_in[b, rows, :].astype(F32)
                    s.stage[b, rows, :] = both.astype(BF16)
                to_owner(b, owner).start()

    def block(f, j, arrived):
        if arrived:
            wait_y(first_down + j, f)
        else:
            have("down")
        b, owner, side = block_of(f, j)
        keep = len(pending) % 2

        def step(r, carry):
            rows = pl.ds(pl.multiple_of(r * n.rows, n.rows), n.rows)
            partial = dot(s.hidden[rows, :], s.wd[f, :, j * LANES : (j + 1) * LANES])

            @pl.when(side == core)
            def _():
                s.kept[keep, rows, :] = partial

            @pl.when(side != core)
            def _():
                s.stage[b, rows, :] = partial.astype(BF16)

            return carry

        lax.fori_loop(0, n.pieces, step, 0)

        @pl.when(side != core)
        def _():
            to_sibling(b).start()

        if pending:
            collect(*pending[-1])
        pending.append((f, j, keep))

    tasks = []

    def at(position, cost, work, *args):
        tasks.append((position, cost, work, args))

    lag = 2.0 / max(last, 1)
    piece_at = [3.0 * r / n.pieces for r in range(n.pieces)]
    for r in range(n.pieces):
        at(0.6 + 2.0 * (r / n.pieces) * 4 / 3, 0.2, tok.forward, r)
        at(1.0 + 2.0 * (r / n.pieces) * 4 / 3, 1.0, norm_one, r)
    for r in range(n.pieces):
        at(3.0, 1.5, mix_in, r)
    for r in range(n.pieces):
        at(3.6, 1.5, conv, r)
    for r in range(n.pieces):
        at(4.3, 0.2, cv.forward, r)
        at(4.3, 2.0, mix_result, r)
    for r in range(n.pieces):
        at(5.3 + 0.45 * r, 0.2, mx.forward, r)
        at(5.6 + 0.45 * r, 1.0, norm_two, r)
    for c in range(len(n.mlp_cols)):
        for r in range(n.pieces):
            at(first_mlp + 2 * (c + 1) + lag, 1.2, mlp_in, c, r)
        for r in range(n.pieces):
            at(first_mlp + 2 * (c + 1) + lag, 0.6, mlp_act, c, r)
    for j in range(n.down_blocks):
        at(0, 1.2, block, fs, j, False)
    for j in range(n.down_blocks):
        for step in range(1, n.shards):
            at(first_down + j + step / max(last, 1) + lag, 1.2, block, arrival(step), j, True)
    drains = [(i + 5.0, drain_chunk, i) for i in range(n.chunks)]
    drains += [(first_down + 0.5, gather.drain, r) for gather in (tok, cv, mx) for r in range(n.pieces)]
    drains.sort(key=lambda entry: entry[0])

    def run_tasks(now, budget):
        while tasks and tasks[0][0] <= now + 1e-6 and budget > 0:
            _, cost, work, args = tasks.pop(0)
            work(*args)
            budget -= cost

    peers = [("tp", (tp + jump) % n.tps) for jump in range(1, n.tps)]
    peers += [("grp", (group + jump) % n.groups) for jump in range(1, n.groups)]
    barrier = pltpu.get_barrier_semaphore()

    def greet(axis, index):
        pl.semaphore_signal(barrier, inc=1, device_id={axis: index}, device_id_type=MESH)

    for axis, index in peers:
        greet(axis, index)

    @pl.when(fs < last)
    def _():
        greet("fs", fs + 1)

    @pl.when(fs > 0)
    def _():
        greet("fs", fs - 1)

    ends = jnp.where(fs == 0, 1, 0) + jnp.where(fs == last, 1, 0)
    pl.semaphore_wait(barrier, len(peers) + 2 - ends)

    for r in range(n.pieces):
        tok.send(r)
        if r < LEAD:
            send_own(r)
    s.glu[:PAD, :] = jnp.zeros((PAD, n.own_channels), F32)
    s.glu[PAD + n.tokens :, :] = jnp.zeros((PAD, n.own_channels), F32)
    for ref in (s.gp, s.up):
        ref[:EDGE, :] = jnp.zeros((EDGE, ref.shape[1]), F32)
        ref[EDGE + n.tokens :, :] = jnp.zeros((EDGE, ref.shape[1]), F32)

    for i in range(n.chunks):
        for step in range(1, n.shards):
            pump(i, step)
            if step == last and i + LEAD < n.chunks:
                send_own(i + LEAD)
            now = i + step / last
            run_tasks(now, BUDGET)
            if drains and drains[0][0] <= now:
                _, work, arg = drains.pop(0)
                work(arg)
    run_tasks(1e9, 1e9)
    collect(*pending[-1])

    have("final_gain")
    for jump in range(1, n.chips):
        for j in range(own_blocks):
            pltpu.make_async_remote_copy(
                src_ref=s.stage.at[0],
                dst_ref=s.own_in.at[jump - 1, j],
                send_sem=s.stage_send.at[0],
                recv_sem=s.own_recv.at[jump - 1, j],
                device_id={"tp": sibling},
                device_id_type=MESH,
            ).wait_recv()

    def sum_up(first):
        rows = pl.ds(first, LANES)
        squares = jnp.zeros((LANES, LANES), F32)
        for j in range(own_blocks):
            columns = slice(j * LANES, (j + 1) * LANES)
            v = s.total[j, rows, :] + s.mx[tp, rows, columns].astype(F32)
            for jump in range(1, n.chips):
                v = v + s.own_in[jump - 1, j, rows, :].astype(F32)
            s.total[j, rows, :] = v
            squares = squares + v * v
        across = jnp.sum(jnp.transpose(squares), axis=0, keepdims=True)
        s.stats[tp, :, rows] = jnp.broadcast_to(across, (8, LANES))

    def each_block(body):
        def step(q, carry):
            body(pl.multiple_of(q * LANES, LANES))
            return carry

        lax.fori_loop(0, n.tokens // LANES, step, 0)

    each_block(sum_up)

    def stats_copy(sender, jump):
        return pltpu.make_async_remote_copy(
            src_ref=s.stats.at[sender],
            dst_ref=s.stats.at[sender],
            send_sem=s.stats_send.at[jump - 1],
            recv_sem=s.stats_recv.at[jump - 1],
            device_id={"tp": (tp + jump) % n.tps},
            device_id_type=MESH,
        )

    for jump in range(1, n.tps):
        stats_copy(tp, jump).start()
    for _, work, arg in drains:
        work(arg)
    for b in range(n.shards * n.down_blocks):
        owner = b // own_blocks

        @pl.when(owner != tp)
        def _():
            to_sibling(b).wait_send()

    for jump in range(1, n.tps):
        stats_copy((tp - jump + n.tps) % n.tps, jump).wait_recv()

    def finish(first):
        rows = pl.ds(first, LANES)
        across = s.stats[0, 0:1, rows]
        for t in range(1, n.tps):
            across = across + s.stats[t, 0:1, rows]
        square = jnp.transpose(jnp.broadcast_to(across, (LANES, LANES)))
        scale = lax.rsqrt(square / n.width + 1e-06)
        for j in range(own_blocks):
            columns = slice(j * LANES, (j + 1) * LANES)
            out[rows, columns] = (s.total[j, rows, :] * scale * s.v_final_gain[:, columns]).astype(BF16)

    each_block(finish)
    for jump in range(1, n.tps):
        stats_copy(tp, jump).wait_send()


def wide(array, axis):
    extra = -array.shape[axis] % LANES
    if not extra:
        return array
    return jnp.pad(array, [(0, extra if k == axis else 0) for k in range(array.ndim)])


INPUTS = (
    "tokens",
    "mix_gain",
    "value",
    "gate",
    "conv_taps",
    "chan_gain",
    "chan_shift",
    "mix",
    "mlp_gain",
    "mgate",
    "mup",
    "gate_taps",
    "up_taps",
    "down",
    "final_gain",
)
SMALL = (
    "mix_gain",
    "conv_taps",
    "chan_gain",
    "chan_shift",
    "mlp_gain",
    "gate_taps",
    "up_taps",
    "final_gain",
)


def local(*values):
    a = dict(zip(INPUTS, values))
    for name in ("mix_gain", "chan_gain", "chan_shift", "mlp_gain", "final_gain"):
        a[name] = a[name][None]
    for name in ("mgate", "mup", "gate_taps", "up_taps"):
        a[name] = wide(a[name], 1)
    a["down"] = wide(a["down"], 0)
    tps, shards, groups = lax.axis_size("tp"), lax.axis_size("fs"), lax.axis_size("grp")
    chips = tps // CORES
    tokens, cols = a["tokens"].shape
    depth, own_channels = a["value"].shape
    hidden = a["mgate"].shape[1]
    mlp_cols = column_chunks(hidden, 3 * LANES)
    down_blocks = a["down"].shape[1] // LANES
    rows = min(256, tokens)
    pieces = tokens // rows
    chunks = 3 + 2 * len(mlp_cols) + down_blocks
    width, channels = cols * tps, own_channels * tps
    blocks = shards * down_blocks
    own_blocks = cols // LANES
    edge = tokens + 2 * EDGE
    vmem, dma = pltpu.VMEM, pltpu.SemaphoreType.DMA
    scratch = {
        "tok": vmem((tps, tokens, cols), BF16),
        "cv": vmem((tps, tokens, own_channels), BF16),
        "mx": vmem((tps, tokens, cols), BF16),
        "xn": vmem((tokens, width), BF16),
        "hm": vmem((tokens, channels), BF16),
        "glu": vmem((tokens + 2 * PAD, own_channels), F32),
        "gp": vmem((edge, mlp_cols[0][1]), F32),
        "up": vmem((edge, mlp_cols[0][1]), F32),
        "hidden": vmem((tokens, hidden), BF16),
        "wv": vmem((width, own_channels), BF16),
        "wg": vmem((width, own_channels), BF16),
        "wm": vmem((channels, cols), BF16),
        "wgate": vmem((width, hidden), BF16),
        "wup": vmem((width, hidden), BF16),
        "wd": vmem((shards,) + a["down"].shape, BF16),
        "kept": vmem((2, tokens, LANES), F32),
        "stage": vmem((blocks, tokens, LANES), BF16),
        "sib_in": vmem((blocks, tokens, LANES), BF16),
        "own_in": vmem((chips - 1, own_blocks, tokens, LANES), BF16),
        "total": vmem((own_blocks, tokens, LANES), F32),
        "stats": vmem((tps, 8, tokens), F32),
        "local_sem": dma((7 + len(SMALL),)),
        "z_recv": dma((chunks, shards)),
        "up_send": dma((chunks, shards)),
        "down_send": dma((chunks, shards)),
        "y_send": dma((groups - 1, chunks, shards)),
        "y_recv": dma((groups - 1, chunks, shards)),
        "gather_send": dma((3, 2 * chips - 1, pieces)),
        "gather_recv": dma((3, tps, pieces)),
        "stage_send": dma((blocks,)),
        "sib_recv": dma((blocks,)),
        "own_recv": dma((chips - 1, own_blocks)),
        "stats_send": dma((tps - 1,)),
        "stats_recv": dma((tps - 1,)),
    }
    for name in SMALL:
        scratch["v_" + name] = vmem(a[name].shape, F32)
    n = SimpleNamespace(
        inputs=INPUTS,
        small=SMALL,
        scratch=tuple(scratch),
        tps=tps,
        shards=shards,
        groups=groups,
        chips=chips,
        tokens=tokens,
        rows=rows,
        pieces=pieces,
        cols=cols,
        width=width,
        channels=channels,
        own_channels=own_channels,
        depth=depth,
        mix_depth=a["mix"].shape[0],
        hidden=hidden,
        mlp_cols=mlp_cols,
        down_blocks=down_blocks,
        chunks=chunks,
        taps=a["conv_taps"].shape[0],
    )
    return pl.pallas_call(
        functools.partial(layer_kernel, n),
        out_shape=jax.ShapeDtypeStruct((tokens, cols), BF16),
        in_specs=[pl.BlockSpec(memory_space=pl.ANY)] * len(INPUTS),
        out_specs=pl.BlockSpec(memory_space=pltpu.VMEM),
        scratch_shapes=list(scratch.values()),
        compiler_params=pltpu.CompilerParams(
            collective_id=0, has_side_effects=True, vmem_limit_bytes=67043328
        ),
        name="layer",
    )(*[a[name] for name in INPUTS])


def solution(mesh):
    return jax.shard_map(
        local,
        mesh=mesh,
        in_specs=(
            P(("grp", "fs"), "tp"),
            P(),
            P("fs", "tp"),
            P("fs", "tp"),
            P(None, "tp"),
            P(),
            P(),
            P("fs", "tp"),
            P(),
            P("fs", "tp"),
            P("fs", "tp"),
            P(None, "tp"),
            P(None, "tp"),
            P("tp", "fs"),
            P("tp"),
        ),
        out_specs=P(("grp", "fs"), "tp"),
        check_vma=False,
    )
```

```python
import functools
from types import SimpleNamespace

import jax
import jax.numpy as jnp
from jax import lax
from jax.experimental import pallas as pl
from jax.experimental.pallas import tpu as pltpu
from jax.sharding import PartitionSpec as P

MESH = pl.DeviceIdType.MESH
F32, BF16 = jnp.float32, jnp.bfloat16
LANES = 128
CORES = 2
LEAD = 2
BLOCK_ROWS = 512
WHOLE = 4
MLP_LAG = 3
DOWN_LAG = 2
PAD = 16
EDGE = 8
BUDGET = 4.5


def column_chunks(width, most):
    return [(first, min(most, width - first)) for first in range(0, width, most)]


def sigmoid(value):
    return 1.0 / (1.0 + jnp.exp(-value))


def layer_kernel(n, *refs):
    arrays = SimpleNamespace(**dict(zip(n.inputs, refs)))
    out = refs[len(n.inputs)]
    s = SimpleNamespace(**dict(zip(n.scratch, refs[len(n.inputs) + 1 :])))

    group, fs, tp = lax.axis_index("grp"), lax.axis_index("fs"), lax.axis_index("tp")
    chip, core = tp // CORES, tp % CORES
    sibling = tp + 1 - 2 * core

    def chip_at(jump):
        return (chip + jump + n.chips) % n.chips

    def rows_of(r):
        return pl.ds(r * n.rows, n.rows)

    local = {}

    def load(name, src, dst):
        index = len(local)
        local[name] = pltpu.make_async_copy(src, dst, s.local_sem.at[index])
        local[name].start()

    loaded = set()

    def have(*names):
        for name in names:
            if name not in loaded:
                loaded.add(name)
                local[name].wait()

    def own_rows(dst, count):
        return dst.at[pl.ds(pl.multiple_of(fs * count, count), count), :]

    load("tokens", arrays.tokens, s.tok.at[tp])
    for name in n.small:
        load(name, getattr(arrays, name), getattr(s, "v_" + name))
    load("value", arrays.value, own_rows(s.wv, n.depth))
    load("gate", arrays.gate, own_rows(s.wg, n.depth))
    load("mix", arrays.mix, own_rows(s.wm, n.mix_depth))
    load("mgate", arrays.mgate, own_rows(s.wgate, n.depth))
    load("mup", arrays.mup, own_rows(s.wup, n.depth))
    load("down", arrays.down, s.wd.at[fs])

    chunks = [
        (arrays.value, s.wv, 0, n.depth, 0, n.own_channels),
        (arrays.gate, s.wg, 0, n.depth, 0, n.own_channels),
        (arrays.mix, s.wm, 0, n.mix_depth, 0, n.cols),
    ]
    first_mlp = len(chunks)
    for first, width in n.mlp_cols:
        chunks.append((arrays.mgate, s.wgate, 0, n.depth, first, width))
        chunks.append((arrays.mup, s.wup, 0, n.depth, first, width))
    first_down = len(chunks)
    for j in range(n.down_blocks):
        count = n.hidden - (n.whole_rows if j == n.down_blocks - 1 else 0)
        chunks.append((arrays.down, s.wd, 0, count, j * LANES, LANES))
    whole = len(chunks)
    chunks.append((arrays.down, s.wd, count, n.whole_rows, j * LANES, LANES))
    assert len(chunks) == n.chunks
    kinds = [0, 1, 2] + [3 + i % 2 for i in range(first_down - first_mlp)]
    kinds += [5] * (n.down_blocks - 1) + [6, 7]

    def part_rows(i, part):
        row, count = chunks[i][2:4]
        if i == whole:
            return row, count
        half = count // n.groups
        return pl.multiple_of(row + part * half, half), half

    def slot(i, f, part):
        _, dst, _, _, first, width = chunks[i]
        row, half = part_rows(i, part)
        columns = pl.ds(first, width)
        if i >= first_down:
            return dst.at[f, pl.ds(row, half), columns]
        return dst.at[pl.ds(pl.multiple_of(f * chunks[i][3] + row, half), half), columns]

    def z_copy(i, f, to, sems, own=False):
        src = slot(i, f, group)
        if own:
            source, _, _, _, first, width = chunks[i]
            row, half = part_rows(i, group)
            src = source.at[pl.ds(row, half), pl.ds(first, width)]
        return pltpu.make_async_remote_copy(
            src_ref=src,
            dst_ref=slot(i, f, group),
            send_sem=sems.at[kinds[i]],
            recv_sem=s.z_recv.at[i, f],
            device_id={"fs": to},
            device_id_type=MESH,
        )

    def y_copy(i, f, jump, part, refs=None):
        refs = slot(i, f, part) if refs is None else refs
        down = i >= first_down
        recv_sem = s.y_down.at[jump - 1, i - first_down, f] if down else s.y_recv.at[jump - 1, i]
        return pltpu.make_async_remote_copy(
            src_ref=refs,
            dst_ref=refs,
            send_sem=s.y_send.at[jump - 1, kinds[i]],
            recv_sem=recv_sem,
            device_id={"grp": (group + jump) % n.groups},
            device_id_type=MESH,
        )

    last = n.shards - 1
    reach = jnp.minimum(fs, last - fs)

    def arrival(step):
        near = fs - (step + 1) // 2 if step % 2 else fs + (step + 1) // 2
        distance = step - reach
        far = jnp.where(fs > last - fs, fs - distance, fs + distance)
        return jnp.where(step <= 2 * reach, near, far)

    def send_own(i):
        @pl.when(fs < last)
        def _():
            z_copy(i, fs, fs + 1, s.up_send, own=True).start()

        @pl.when(fs > 0)
        def _():
            z_copy(i, fs, fs - 1, s.down_send, own=True).start()

    def pump(i, step):
        f = arrival(step)
        z_copy(i, f, fs, s.up_send).wait_recv()

        @pl.when(jnp.logical_and(f < fs, fs < last))
        def _():
            z_copy(i, f, fs + 1, s.up_send).start()

        @pl.when(jnp.logical_and(f > fs, fs > 0))
        def _():
            z_copy(i, f, fs - 1, s.down_send).start()

        for jump in range(1, n.groups if i != whole else 1):
            y_copy(i, f, jump, group).start()

    def wait_y(i, f):
        for jump in range(1, n.groups):
            y_copy(i, f, jump, (group - jump + n.groups) % n.groups).wait_recv()

    def ready(i):
        _, dst, _, depth, first, width = chunks[i]
        refs = dst.at[pl.ds(0, last * (depth // n.groups)), pl.ds(first, width)]
        for jump in range(1, n.groups):
            y_copy(i, fs, jump, group, refs).wait_recv()

    def sent(kind, count):
        i = kinds.index(kind)
        _, dst, _, depth, _, _ = chunks[i]
        half = depth if kind == 7 else depth // n.groups
        if kind < 5:
            return i, dst.at[pl.ds(0, count * half), :]
        columns = (n.down_blocks - 1 if kind == 5 else 1) * LANES
        return i, dst.at[pl.ds(0, count), pl.ds(0, half), pl.ds(0, columns)]

    def drain():
        def wait(sems, to, count, kind):
            i, refs = sent(kind, count)
            pltpu.make_async_remote_copy(
                src_ref=refs,
                dst_ref=refs,
                send_sem=sems.at[kind],
                recv_sem=s.z_recv.at[0, 0],
                device_id={"fs": to},
                device_id_type=MESH,
            ).wait_send()

        used = sorted(set(kinds))
        for count in range(1, n.shards):

            @pl.when(fs + 1 == count)
            def _():
                for kind in used:
                    wait(s.up_send, fs + 1, count, kind)

            @pl.when(last - fs + 1 == count)
            def _():
                for kind in used:
                    wait(s.down_send, fs - 1, count, kind)

        for kind in used[:-1]:
            i, refs = sent(kind, last)
            for jump in range(1, n.groups):
                y_copy(i, fs, jump, group, refs).wait_send()

    class Gather:
        def __init__(self, blocks, kind, own=None):
            self.blocks, self.kind, self.own = blocks, kind, own

        def copy(self, block, r, to, jump, src=None):
            dst = self.blocks.at[block, rows_of(r), :]
            sems = s.gather_chip.at[self.kind, jump - 1, r] if jump else s.gather_core.at[self.kind, r]
            return pltpu.make_async_remote_copy(
                src_ref=dst if src is None else src,
                dst_ref=dst,
                send_sem=s.gather_send.at[self.kind],
                recv_sem=sems,
                device_id={"tp": to},
                device_id_type=MESH,
            )

        def send(self, r):
            src = None if self.own is None else self.own.at[rows_of(r), :]
            for jump in range(1, n.chips):
                self.copy(tp, r, chip_at(jump) * CORES + core, jump, src).start()
            self.copy(tp, r, sibling, 0, src).start()

        def forward(self, r):
            for jump in range(1, n.chips):
                block = chip_at(-jump) * CORES + core
                self.copy(block, r, sibling, jump).wait_recv()
                self.copy(block, r, sibling, 0).start()

        def wait(self, r):
            refs = self.blocks.at[pl.ds(0, n.chips), rows_of(r), :]
            pltpu.make_async_remote_copy(
                src_ref=refs,
                dst_ref=refs,
                send_sem=s.gather_send.at[self.kind],
                recv_sem=s.gather_core.at[self.kind, r],
                device_id={"tp": sibling},
                device_id_type=MESH,
            ).wait_recv()

        def drain(self):
            refs = self.blocks.at[pl.ds(0, 2 * n.chips - 1)]
            pltpu.make_async_remote_copy(
                src_ref=refs,
                dst_ref=refs,
                send_sem=s.gather_send.at[self.kind],
                recv_sem=s.gather_core.at[self.kind, 0],
                device_id={"tp": sibling},
                device_id_type=MESH,
            ).wait_send()

    tok = Gather(s.tok, 0, arrays.tokens)
    cv = Gather(s.cv, 1)
    mx = Gather(s.mx, 2)

    def each_tile(r, size, body):
        def step(q, carry):
            body(pl.multiple_of(r * n.rows + q * size, size))
            return carry

        lax.fori_loop(0, n.rows // size, step, 0)

    def norm_rows(blocks, gain, r):
        def body(first):
            rows = pl.ds(first, 32)
            total = jnp.zeros((32, 1), F32)
            for t in range(n.tps):
                v = blocks[t, rows, :].astype(F32)
                total = total + jnp.sum(v * v, axis=-1, keepdims=True)
            scale = lax.rsqrt(total / n.width + 1e-06)
            for t in range(n.tps):
                columns = slice(t * n.cols, (t + 1) * n.cols)
                v = blocks[t, rows, :].astype(F32)
                s.xn[rows, columns] = (v * scale * gain[:, columns]).astype(BF16)

        each_tile(r, 32, body)

    def dot(a, b):
        return jnp.dot(a, b, preferred_element_type=F32)

    def norm_one(r):
        have("tokens", "mix_gain")
        tok.wait(r)
        norm_rows(s.tok, s.v_mix_gain, r)

    def mix_in(r):
        if r == 0:
            have("value", "gate", "conv_taps")
            ready(0)
            ready(1)
        x = s.xn[rows_of(r), :]
        value = dot(x, s.wv[...])
        gate = dot(x, s.wg[...])
        s.glu[pl.ds(PAD + r * n.rows, n.rows), :] = value * sigmoid(gate)

    def conv(r):
        tile, half = 64, (n.taps - 1) // 2
        window = tile + 2 * PAD
        for lanes in range(0, n.own_channels, LANES):
            columns = slice(lanes, lanes + LANES)

            def body(first):
                x = s.glu[pl.ds(first, window), columns]
                total = jnp.zeros((tile, LANES), F32)
                for shift in range(8):
                    moved = pltpu.roll(x, window - shift, 0) if shift else x
                    for k in range(n.taps):
                        at = PAD - half + k
                        if at % 8 == shift:
                            piece = moved[at - shift : at - shift + tile]
                            total = total + s.v_conv_taps[k : k + 1, columns] * piece
                s.cv[tp, pl.ds(first, tile), columns] = total.astype(BF16)

            each_tile(r, tile, body)
        cv.send(r)

    def mix_result(r):
        if r == 0:
            have("chan_gain", "chan_shift", "mix")
            ready(2)
        cv.wait(r)

        def body(first):
            rows = pl.ds(first, 32)
            total = jnp.zeros((32, 1), F32)
            square = jnp.zeros((32, 1), F32)
            for t in range(n.tps):
                v = s.cv[t, rows, :].astype(F32)
                total = total + jnp.sum(v, axis=-1, keepdims=True)
                square = square + jnp.sum(v * v, axis=-1, keepdims=True)
            mean = total / n.channels
            scale = lax.rsqrt(square / n.channels - mean * mean + 1e-05)
            for t in range(n.tps):
                columns = slice(t * n.own_channels, (t + 1) * n.own_channels)
                v = s.cv[t, rows, :].astype(F32)
                v = (v - mean) * scale * s.v_chan_gain[:, columns] + s.v_chan_shift[:, columns]
                s.hm[rows, columns] = (v * sigmoid(v)).astype(BF16)

        each_tile(r, 32, body)
        rows = rows_of(r)
        result = dot(s.hm[rows, :], s.wm[...])
        s.mx[tp, rows, :] = (s.tok[tp, rows, :].astype(F32) + result).astype(BF16)
        mx.send(r)

    def norm_two(r):
        have("mlp_gain")
        mx.wait(r)
        norm_rows(s.mx, s.v_mlp_gain, r)

    def mlp_in(c, r):
        first, width = n.mlp_cols[c]
        if r == 0:
            have("mgate", "mup", "gate_taps", "up_taps")
            ready(first_mlp + 2 * c)
            ready(first_mlp + 2 * c + 1)
        x = s.xn[rows_of(r), :]
        rows = pl.ds(EDGE + r * n.rows, n.rows)
        s.gp[rows, :width] = dot(x, s.wgate[:, first : first + width])
        s.up[rows, :width] = dot(x, s.wup[:, first : first + width])

    def mlp_act(c, r):
        first_column, width = n.mlp_cols[c]
        tile = 32
        window = tile + 2 * EDGE

        def filtered(values, taps, first, lanes, columns):
            x = values[pl.ds(first, window), lanes : lanes + LANES]
            low = pltpu.roll(x, 1, 0)[EDGE : EDGE + tile]
            high = pltpu.roll(x, window - 1, 0)[EDGE : EDGE + tile]
            middle = x[EDGE : EDGE + tile]
            return taps[0:1, columns] * low + taps[1:2, columns] * middle + taps[2:3, columns] * high

        def body(first):
            for lanes in range(0, width, LANES):
                columns = slice(first_column + lanes, first_column + lanes + LANES)
                gate = filtered(s.gp, s.v_gate_taps, first, lanes, columns)
                up = filtered(s.up, s.v_up_taps, first, lanes, columns)
                s.hidden[pl.ds(first, tile), columns] = (gate * sigmoid(gate) * up).astype(BF16)

        each_tile(r, tile, body)

    own_blocks = n.cols // LANES
    pending = []

    def block_of(f, j):
        b = f * n.down_blocks + j
        owner = b // own_blocks
        return b, owner, owner % CORES

    def sib_index(b):
        return b // own_blocks // CORES * own_blocks + b % own_blocks

    def block_rows(r):
        return pl.ds(pl.multiple_of(r * n.block_rows, n.block_rows), n.block_rows)

    def to_sibling(b, r):
        return pltpu.make_async_remote_copy(
            src_ref=s.stage.at[b, block_rows(r)],
            dst_ref=s.sib_in.at[sib_index(b), block_rows(r)],
            send_sem=s.stage_send.at[0],
            recv_sem=s.sib_recv.at[sib_index(b), r],
            device_id={"tp": sibling},
            device_id_type=MESH,
        )

    def to_owner(b, r, owner, index):
        return pltpu.make_async_remote_copy(
            src_ref=s.stage.at[b, block_rows(r)],
            dst_ref=s.own_in.at[index, b % own_blocks, block_rows(r)],
            send_sem=s.stage_send.at[0],
            recv_sem=s.own_recv.at[index, b % own_blocks, r],
            device_id={"tp": owner},
            device_id_type=MESH,
        )

    def each_piece(body):
        def step(r, carry):
            body(r, block_rows(r))
            return carry

        lax.fori_loop(0, n.tokens // n.block_rows, step, 0)

    def collect(f, j, keep):
        b, owner, side = block_of(f, j)
        jump = (chip - owner // CORES + n.chips) % n.chips
        index = jnp.maximum(jump - 1, 0)

        @pl.when(jnp.logical_and(side == core, owner == tp))
        def _():
            def body(r, rows):
                to_sibling(b, r).wait_recv()
                s.total[b % own_blocks, rows, :] = s.kept[keep, rows, :] + s.sib_in[sib_index(b), rows, :].astype(F32)

            each_piece(body)

        @pl.when(jnp.logical_and(side == core, owner != tp))
        def _():
            def body(r, rows):
                to_sibling(b, r).wait_recv()
                both = s.kept[keep, rows, :] + s.sib_in[sib_index(b), rows, :].astype(F32)
                s.stage[b, rows, :] = both.astype(BF16)
                to_owner(b, r, owner, index).start()

            each_piece(body)

    def block(f, j, step):
        last_columns = j == n.down_blocks - 1
        if step == 0:
            have("down")
        elif not last_columns:
            wait_y(first_down + j, f)
        b, owner, side = block_of(f, j)
        keep = len(pending) % 2
        columns = slice(j * LANES, (j + 1) * LANES)

        def body(r, rows):
            if step and last_columns:
                partial = s.early[step - 1, rows, :] + dot(s.hidden[rows, count:], s.wd[f, count:, columns])
            else:
                partial = dot(s.hidden[rows, :], s.wd[f, :, columns])

            @pl.when(side == core)
            def _():
                s.kept[keep, rows, :] = partial

            @pl.when(side != core)
            def _():
                s.stage[b, rows, :] = partial.astype(BF16)
                to_sibling(b, r).start()

        each_piece(body)
        if pending:
            collect(*pending[-1])
        pending.append((f, j, keep))

    def early(f, j, step):
        wait_y(first_down + j, f)
        columns = slice(j * LANES, (j + 1) * LANES)

        def body(r, rows):
            s.early[step - 1, rows, :] = dot(s.hidden[rows, :count], s.wd[f, :count, columns])

        each_piece(body)

    tasks = []

    def at(position, cost, work, *args):
        tasks.append((position, cost, work, args))

    def beats(count):
        return count / max(last, 1)

    for r in range(n.pieces):
        at(0.6 + 2.0 * (r / n.pieces) * 4 / 3, 0.2, tok.forward, r)
        at(1.0 + 2.0 * (r / n.pieces) * 4 / 3, 1.0, norm_one, r)
    for r in range(n.pieces):
        at(3.0, 1.5, mix_in, r)
    for r in range(n.pieces):
        at(3.6, 1.5, conv, r)
    for r in range(n.pieces):
        at(4.3 + 0.33 * r, 0.2, cv.forward, r)
        at(4.6 + 0.33 * r, 4.0, mix_result, r)
    for r in range(n.pieces):
        at(5.6 + 0.45 * r, 0.2, mx.forward, r)
        at(5.9 + 0.45 * r, 1.0, norm_two, r)
    for c in range(len(n.mlp_cols)):
        ready_at = first_mlp + 2 * (c + 1) + beats(n.mlp_lag)
        for r in range(n.pieces):
            at(ready_at, 1.2, mlp_in, c, r)
        for r in range(n.pieces):
            at(ready_at, 0.6, mlp_act, c, r)
    for j in range(n.down_blocks):
        at(0, 1.2, block, fs, j, 0)
    for j in range(n.down_blocks):
        work = block if j < n.down_blocks - 1 else early
        for step in range(1, n.shards):
            at(first_down + j + beats(step + n.down_lag), 1.2, work, arrival(step), j, step)
    for step in range(1, n.shards):
        at(whole + beats(step), 1.2, block, arrival(step), j, step)
    def run_tasks(now, budget):
        while tasks and tasks[0][0] <= now + 1e-6 and budget > 0:
            _, cost, work, args = tasks.pop(0)
            work(*args)
            budget -= cost

    peers = [("tp", (tp + jump) % n.tps) for jump in range(1, n.tps)]
    peers += [("grp", (group + jump) % n.groups) for jump in range(1, n.groups)]
    barrier = pltpu.get_barrier_semaphore()

    def greet(axis, index):
        pl.semaphore_signal(barrier, inc=1, device_id={axis: index}, device_id_type=MESH)

    for axis, index in peers:
        greet(axis, index)

    @pl.when(fs < last)
    def _():
        greet("fs", fs + 1)

    @pl.when(fs > 0)
    def _():
        greet("fs", fs - 1)

    ends = jnp.where(fs == 0, 1, 0) + jnp.where(fs == last, 1, 0)
    pl.semaphore_wait(barrier, len(peers) + 2 - ends)

    for r in range(n.pieces):
        tok.send(r)
        if r < LEAD:
            send_own(r)
    s.glu[:PAD, :] = jnp.zeros((PAD, n.own_channels), F32)
    s.glu[PAD + n.tokens :, :] = jnp.zeros((PAD, n.own_channels), F32)
    for ref in (s.gp, s.up):
        ref[:EDGE, :] = jnp.zeros((EDGE, ref.shape[1]), F32)
        ref[EDGE + n.tokens :, :] = jnp.zeros((EDGE, ref.shape[1]), F32)

    at_end = reach == 0

    def pump_own(i):
        pump(i, 1)

    for i in range(min(LEAD, n.chunks)):
        pl.when(at_end)(functools.partial(pump_own, i))
    for i in range(n.chunks):
        pl.when(jnp.logical_not(at_end))(functools.partial(pump_own, i))
        run_tasks(i + 1 / last, BUDGET)
        for step in range(2, n.shards):
            pump(i, step)
            if step < last:
                run_tasks(i + step / last, BUDGET)
        if i + LEAD < n.chunks:
            send_own(i + LEAD)
            pl.when(at_end)(functools.partial(pump_own, i + LEAD))
        run_tasks(i + 1.0, BUDGET)
    run_tasks(1e9, 1e9)
    collect(*pending[-1])

    have("final_gain")

    def sum_up(first):
        rows = pl.ds(first, LANES)
        squares = jnp.zeros((LANES, LANES), F32)
        for j in range(own_blocks):
            columns = slice(j * LANES, (j + 1) * LANES)
            v = s.total[j, rows, :] + s.mx[tp, rows, columns].astype(F32)
            for jump in range(1, n.chips):
                v = v + s.own_in[jump - 1, j, rows, :].astype(F32)
            s.total[j, rows, :] = v
            squares = squares + v * v
        across = jnp.sum(jnp.transpose(squares), axis=0, keepdims=True)
        s.stats[tp, :, rows] = jnp.broadcast_to(across, (8, LANES))

    def sum_piece(r, rows):
        for jump in range(1, n.chips):
            for j in range(own_blocks):
                to_owner(j, r, sibling, jump - 1).wait_recv()
        for first in range(0, n.block_rows, LANES):
            sum_up(pl.multiple_of(r * n.block_rows + first, LANES))

    def each_block(body):
        def step(q, carry):
            body(pl.multiple_of(q * LANES, LANES))
            return carry

        lax.fori_loop(0, n.tokens // LANES, step, 0)

    each_piece(sum_piece)

    def stats_copy(refs, jump):
        return pltpu.make_async_remote_copy(
            src_ref=refs,
            dst_ref=refs,
            send_sem=s.stats_send.at[0],
            recv_sem=s.stats_recv.at[0],
            device_id={"tp": (tp + jump) % n.tps},
            device_id_type=MESH,
        )

    for jump in range(1, n.tps):
        stats_copy(s.stats.at[tp], jump).start()
    drain()
    for gather in (tok, cv, mx):
        gather.drain()
    refs = s.stage.at[pl.ds(0, n.shards * n.down_blocks - own_blocks)]
    pltpu.make_async_remote_copy(
        src_ref=refs,
        dst_ref=refs,
        send_sem=s.stage_send.at[0],
        recv_sem=s.stats_recv.at[0],
        device_id={"tp": sibling},
        device_id_type=MESH,
    ).wait_send()
    all_stats = s.stats.at[pl.ds(0, n.tps - 1)]
    stats_copy(all_stats, 1).wait_recv()

    def finish(first):
        rows = pl.ds(first, LANES)
        across = s.stats[0, 0:1, rows]
        for t in range(1, n.tps):
            across = across + s.stats[t, 0:1, rows]
        square = jnp.transpose(jnp.broadcast_to(across, (LANES, LANES)))
        scale = lax.rsqrt(square / n.width + 1e-06)
        for j in range(own_blocks):
            columns = slice(j * LANES, (j + 1) * LANES)
            out[rows, columns] = (s.total[j, rows, :] * scale * s.v_final_gain[:, columns]).astype(BF16)

    each_block(finish)
    stats_copy(all_stats, 1).wait_send()


def wide(array, axis):
    extra = -array.shape[axis] % LANES
    if not extra:
        return array
    return jnp.pad(array, [(0, extra if k == axis else 0) for k in range(array.ndim)])


INPUTS = (
    "tokens",
    "mix_gain",
    "value",
    "gate",
    "conv_taps",
    "chan_gain",
    "chan_shift",
    "mix",
    "mlp_gain",
    "mgate",
    "mup",
    "gate_taps",
    "up_taps",
    "down",
    "final_gain",
)
SMALL = (
    "mix_gain",
    "conv_taps",
    "chan_gain",
    "chan_shift",
    "mlp_gain",
    "gate_taps",
    "up_taps",
    "final_gain",
)


def local(*values):
    a = dict(zip(INPUTS, values))
    for name in ("mix_gain", "chan_gain", "chan_shift", "mlp_gain", "final_gain"):
        a[name] = a[name][None]
    for name in ("mgate", "mup", "gate_taps", "up_taps"):
        a[name] = wide(a[name], 1)
    a["down"] = wide(a["down"], 0)
    tps, shards, groups = lax.axis_size("tp"), lax.axis_size("fs"), lax.axis_size("grp")
    chips = tps // CORES
    tokens, cols = a["tokens"].shape
    depth, own_channels = a["value"].shape
    hidden = a["mgate"].shape[1]
    mlp_cols = column_chunks(hidden, 3 * LANES)
    down_blocks = a["down"].shape[1] // LANES
    rows = min(256, tokens)
    pieces = tokens // rows
    block_rows = min(BLOCK_ROWS, tokens)
    chunks = 4 + 2 * len(mlp_cols) + down_blocks
    whole_rows = hidden * WHOLE // 8 // LANES * LANES
    width, channels = cols * tps, own_channels * tps
    blocks = shards * down_blocks
    own_blocks = cols // LANES
    edge = tokens + 2 * EDGE
    vmem, dma = pltpu.VMEM, pltpu.SemaphoreType.DMA
    scratch = {
        "tok": vmem((tps, tokens, cols), BF16),
        "cv": vmem((tps, tokens, own_channels), BF16),
        "mx": vmem((tps, tokens, cols), BF16),
        "xn": vmem((tokens, width), BF16),
        "hm": vmem((tokens, channels), BF16),
        "glu": vmem((tokens + 2 * PAD, own_channels), F32),
        "gp": vmem((edge, mlp_cols[0][1]), F32),
        "up": vmem((edge, mlp_cols[0][1]), F32),
        "hidden": vmem((tokens, hidden), BF16),
        "wv": vmem((width, own_channels), BF16),
        "wg": vmem((width, own_channels), BF16),
        "wm": vmem((channels, cols), BF16),
        "wgate": vmem((width, hidden), BF16),
        "wup": vmem((width, hidden), BF16),
        "wd": vmem((shards,) + a["down"].shape, BF16),
        "early": vmem((shards - 1, tokens, LANES), F32),
        "kept": vmem((2, tokens, LANES), F32),
        "stage": vmem((blocks, tokens, LANES), BF16),
        "sib_in": vmem((blocks // CORES, tokens, LANES), BF16),
        "own_in": vmem((chips - 1, own_blocks, tokens, LANES), BF16),
        "total": vmem((own_blocks, tokens, LANES), F32),
        "stats": vmem((tps, 8, tokens), F32),
        "local_sem": dma((7 + len(SMALL),)),
        "z_recv": dma((chunks, shards)),
        "up_send": dma((8,)),
        "down_send": dma((8,)),
        "y_send": dma((groups - 1, 8)),
        "y_recv": dma((groups - 1, chunks - down_blocks - 1)),
        "y_down": dma((groups - 1, down_blocks, shards)),
        "gather_send": dma((3,)),
        "gather_chip": dma((3, chips - 1, pieces)),
        "gather_core": dma((3, pieces)),
        "stage_send": dma((1,)),
        "sib_recv": dma((blocks // CORES, tokens // block_rows)),
        "own_recv": dma((chips - 1, own_blocks, tokens // block_rows)),
        "stats_send": dma((1,)),
        "stats_recv": dma((1,)),
    }
    for name in SMALL:
        scratch["v_" + name] = vmem(a[name].shape, F32)
    n = SimpleNamespace(
        inputs=INPUTS,
        small=SMALL,
        scratch=tuple(scratch),
        tps=tps,
        shards=shards,
        groups=groups,
        chips=chips,
        tokens=tokens,
        rows=rows,
        pieces=pieces,
        block_rows=block_rows,
        cols=cols,
        width=width,
        channels=channels,
        own_channels=own_channels,
        depth=depth,
        mix_depth=a["mix"].shape[0],
        hidden=hidden,
        mlp_cols=mlp_cols,
        down_blocks=down_blocks,
        whole_rows=whole_rows,
        mlp_lag=MLP_LAG,
        down_lag=DOWN_LAG,
        chunks=chunks,
        taps=a["conv_taps"].shape[0],
    )
    return pl.pallas_call(
        functools.partial(layer_kernel, n),
        out_shape=jax.ShapeDtypeStruct((tokens, cols), BF16),
        in_specs=[pl.BlockSpec(memory_space=pl.ANY)] * len(INPUTS),
        out_specs=pl.BlockSpec(memory_space=pltpu.VMEM),
        scratch_shapes=list(scratch.values()),
        compiler_params=pltpu.CompilerParams(
            collective_id=0, has_side_effects=True, vmem_limit_bytes=67043328
        ),
        name="layer",
    )(*[a[name] for name in INPUTS])


def solution(mesh):
    return jax.shard_map(
        local,
        mesh=mesh,
        in_specs=(
            P(("grp", "fs"), "tp"),
            P(),
            P("fs", "tp"),
            P("fs", "tp"),
            P(None, "tp"),
            P(),
            P(),
            P("fs", "tp"),
            P(),
            P("fs", "tp"),
            P("fs", "tp"),
            P(None, "tp"),
            P(None, "tp"),
            P("tp", "fs"),
            P("tp"),
        ),
        out_specs=P(("grp", "fs"), "tp"),
        check_vma=False,
    )
```

```python
import functools
from types import SimpleNamespace

import jax
import jax.numpy as jnp
from jax import lax
from jax.experimental import pallas as pl
from jax.experimental.pallas import tpu as pltpu
from jax.sharding import PartitionSpec as P

MESH = pl.DeviceIdType.MESH
F32, BF16 = jnp.float32, jnp.bfloat16
LANES = 128
CORES = 2
LEAD = 2
BLOCK_ROWS = 512
GRANT = 67043328
WHOLE = 4
MLP_LAG = 4
DOWN_LAG = 3
OWN_AHEAD = 5
PAD = 16
EDGE = 8
BUDGET = 4.5


def column_chunks(width, most):
    return [(first, min(most, width - first)) for first in range(0, width, most)]


def sigmoid(value):
    return 1.0 / (1.0 + jnp.exp(-value))


def layer_kernel(n, *refs):
    arrays = SimpleNamespace(**dict(zip(n.inputs, refs)))
    out = refs[len(n.inputs)]
    s = SimpleNamespace(**dict(zip(n.scratch, refs[len(n.inputs) + 1 :])))

    group, fs, tp = lax.axis_index("grp"), lax.axis_index("fs"), lax.axis_index("tp")
    chip, core = tp // CORES, tp % CORES
    sibling = tp + 1 - 2 * core

    def chip_at(jump):
        return (chip + jump + n.chips) % n.chips

    def rows_of(r):
        return pl.ds(r * n.rows, n.rows)

    local = {}

    def load(name, src, dst):
        index = len(local)
        local[name] = pltpu.make_async_copy(src, dst, s.local_sem.at[index])
        local[name].start()

    loaded = set()

    def have(*names):
        for name in names:
            if name not in loaded:
                loaded.add(name)
                local[name].wait()

    def own_rows(dst, count):
        return dst.at[pl.ds(pl.multiple_of(fs * count, count), count), :]

    load("tokens", arrays.tokens, s.tok.at[tp])
    for name in n.small:
        load(name, getattr(arrays, name), getattr(s, "v_" + name))
    load("value", arrays.value, own_rows(s.wv, n.depth))
    load("gate", arrays.gate, own_rows(s.wg, n.depth))
    load("mix", arrays.mix, own_rows(s.wm, n.mix_depth))
    load("mgate", arrays.mgate, own_rows(s.wgate, n.depth))
    load("mup", arrays.mup, own_rows(s.wup, n.depth))
    load("down", arrays.down, s.wd.at[fs])

    chunks = [
        (arrays.value, s.wv, 0, n.depth, 0, n.own_channels),
        (arrays.gate, s.wg, 0, n.depth, 0, n.own_channels),
        (arrays.mix, s.wm, 0, n.mix_depth, 0, n.cols),
    ]
    first_mlp = len(chunks)
    for first, width in n.mlp_cols:
        chunks.append((arrays.mgate, s.wgate, 0, n.depth, first, width))
        chunks.append((arrays.mup, s.wup, 0, n.depth, first, width))
    first_down = len(chunks)
    for j in range(n.down_blocks):
        count = n.hidden - (n.whole_rows if j == n.down_blocks - 1 else 0)
        chunks.append((arrays.down, s.wd, 0, count, j * LANES, LANES))
    whole = len(chunks)
    chunks.append((arrays.down, s.wd, count, n.whole_rows, j * LANES, LANES))
    assert len(chunks) == n.chunks
    kinds = [0, 1, 2] + [3 + i % 2 for i in range(first_down - first_mlp)]
    kinds += [5] * (n.down_blocks - 1) + [6, 7]

    def part_rows(i, part):
        row, count = chunks[i][2:4]
        if i == whole:
            return row, count
        half = count // n.groups
        return pl.multiple_of(row + part * half, half), half

    def slot(i, f, part):
        _, dst, _, _, first, width = chunks[i]
        row, half = part_rows(i, part)
        columns = pl.ds(first, width)
        if i >= first_down:
            return dst.at[f, pl.ds(row, half), columns]
        return dst.at[pl.ds(pl.multiple_of(f * chunks[i][3] + row, half), half), columns]

    def z_copy(i, f, to, sems, own=False):
        src = slot(i, f, group)
        if own:
            source, _, _, _, first, width = chunks[i]
            row, half = part_rows(i, group)
            src = source.at[pl.ds(row, half), pl.ds(first, width)]
        return pltpu.make_async_remote_copy(
            src_ref=src,
            dst_ref=slot(i, f, group),
            send_sem=sems.at[kinds[i]],
            recv_sem=s.z_recv.at[i, f],
            device_id={"fs": to},
            device_id_type=MESH,
        )

    def y_copy(i, f, jump, part, refs=None):
        refs = slot(i, f, part) if refs is None else refs
        down = i >= first_down
        recv_sem = s.y_down.at[jump - 1, i - first_down, f] if down else s.y_recv.at[jump - 1, i]
        return pltpu.make_async_remote_copy(
            src_ref=refs,
            dst_ref=refs,
            send_sem=s.y_send.at[jump - 1, kinds[i]],
            recv_sem=recv_sem,
            device_id={"grp": (group + jump) % n.groups},
            device_id_type=MESH,
        )

    last = n.shards - 1
    reach = jnp.minimum(fs, last - fs)

    def arrival(step):
        near = fs - (step + 1) // 2 if step % 2 else fs + (step + 1) // 2
        distance = step - reach
        far = jnp.where(fs > last - fs, fs - distance, fs + distance)
        return jnp.where(step <= 2 * reach, near, far)

    def send_own(i):
        @pl.when(fs < last)
        def _():
            z_copy(i, fs, fs + 1, s.up_send, own=True).start()

        @pl.when(fs > 0)
        def _():
            z_copy(i, fs, fs - 1, s.down_send, own=True).start()

    def pump(i, step):
        f = arrival(step)
        z_copy(i, f, fs, s.up_send).wait_recv()

        @pl.when(jnp.logical_and(f < fs, fs < last))
        def _():
            z_copy(i, f, fs + 1, s.up_send).start()

        @pl.when(jnp.logical_and(f > fs, fs > 0))
        def _():
            z_copy(i, f, fs - 1, s.down_send).start()

        for jump in range(1, n.groups if i != whole else 1):
            y_copy(i, f, jump, group).start()

    def wait_y(i, f):
        for jump in range(1, n.groups):
            y_copy(i, f, jump, (group - jump + n.groups) % n.groups).wait_recv()

    def ready(i):
        _, dst, _, depth, first, width = chunks[i]
        refs = dst.at[pl.ds(0, last * (depth // n.groups)), pl.ds(first, width)]
        for jump in range(1, n.groups):
            y_copy(i, fs, jump, group, refs).wait_recv()

    def sent(kind, count):
        i = kinds.index(kind)
        _, dst, _, depth, _, _ = chunks[i]
        half = depth if kind == 7 else depth // n.groups
        if kind < 5:
            return i, dst.at[pl.ds(0, count * half), :]
        columns = (n.down_blocks - 1 if kind == 5 else 1) * LANES
        return i, dst.at[pl.ds(0, count), pl.ds(0, half), pl.ds(0, columns)]

    def drain():
        def wait(sems, to, count, kind):
            i, refs = sent(kind, count)
            pltpu.make_async_remote_copy(
                src_ref=refs,
                dst_ref=refs,
                send_sem=sems.at[kind],
                recv_sem=s.z_recv.at[0, 0],
                device_id={"fs": to},
                device_id_type=MESH,
            ).wait_send()

        used = sorted(set(kinds))
        for count in range(1, n.shards):

            @pl.when(fs + 1 == count)
            def _():
                for kind in used:
                    wait(s.up_send, fs + 1, count, kind)

            @pl.when(last - fs + 1 == count)
            def _():
                for kind in used:
                    wait(s.down_send, fs - 1, count, kind)

        for kind in used[:-1]:
            i, refs = sent(kind, last)
            for jump in range(1, n.groups):
                y_copy(i, fs, jump, group, refs).wait_send()

    class Gather:
        def __init__(self, blocks, kind, own=None):
            self.blocks, self.kind, self.own = blocks, kind, own

        def copy(self, block, r, to, jump, src=None):
            dst = self.blocks.at[block, rows_of(r), :]
            sems = s.gather_chip.at[self.kind, jump - 1, r] if jump else s.gather_core.at[self.kind, r]
            return pltpu.make_async_remote_copy(
                src_ref=dst if src is None else src,
                dst_ref=dst,
                send_sem=s.gather_send.at[self.kind],
                recv_sem=sems,
                device_id={"tp": to},
                device_id_type=MESH,
            )

        def send(self, r):
            src = None if self.own is None else self.own.at[rows_of(r), :]
            for jump in range(1, n.chips):
                self.copy(tp, r, chip_at(jump) * CORES + core, jump, src).start()
            self.copy(tp, r, sibling, 0, src).start()

        def forward(self, r):
            for jump in range(1, n.chips):
                block = chip_at(-jump) * CORES + core
                self.copy(block, r, sibling, jump).wait_recv()
                self.copy(block, r, sibling, 0).start()

        def wait(self, r):
            refs = self.blocks.at[pl.ds(0, n.chips), rows_of(r), :]
            pltpu.make_async_remote_copy(
                src_ref=refs,
                dst_ref=refs,
                send_sem=s.gather_send.at[self.kind],
                recv_sem=s.gather_core.at[self.kind, r],
                device_id={"tp": sibling},
                device_id_type=MESH,
            ).wait_recv()

        def drain(self):
            refs = self.blocks.at[pl.ds(0, 2 * n.chips - 1)]
            pltpu.make_async_remote_copy(
                src_ref=refs,
                dst_ref=refs,
                send_sem=s.gather_send.at[self.kind],
                recv_sem=s.gather_core.at[self.kind, 0],
                device_id={"tp": sibling},
                device_id_type=MESH,
            ).wait_send()

    tok = Gather(s.tok, 0, arrays.tokens)
    cv = Gather(s.cv, 1)
    mx = Gather(s.mx, 2)

    def each_tile(r, size, body):
        def step(q, carry):
            body(pl.multiple_of(r * n.rows + q * size, size))
            return carry

        lax.fori_loop(0, n.rows // size, step, 0)

    def norm_rows(blocks, gain, r):
        def body(first):
            rows = pl.ds(first, 32)
            total = jnp.zeros((32, 1), F32)
            for t in range(n.tps):
                v = blocks[t, rows, :].astype(F32)
                total = total + jnp.sum(v * v, axis=-1, keepdims=True)
            scale = lax.rsqrt(total / n.width + 1e-06)
            for t in range(n.tps):
                columns = slice(t * n.cols, (t + 1) * n.cols)
                v = blocks[t, rows, :].astype(F32)
                s.xn[rows, columns] = (v * scale * gain[:, columns]).astype(BF16)

        each_tile(r, 32, body)

    def dot(a, b):
        return jnp.dot(a, b, preferred_element_type=F32)

    def norm_one(r):
        have("tokens", "mix_gain")
        tok.wait(r)
        norm_rows(s.tok, s.v_mix_gain, r)

    def mix_in(r):
        if r == 0:
            have("value", "gate", "conv_taps")
            ready(0)
            ready(1)
        x = s.xn[rows_of(r), :]
        value = dot(x, s.wv[...])
        gate = dot(x, s.wg[...])
        s.glu[pl.ds(PAD + r * n.rows, n.rows), :] = value * sigmoid(gate)

    def conv(r):
        tile, half = 64, (n.taps - 1) // 2
        window = tile + 2 * PAD
        for lanes in range(0, n.own_channels, LANES):
            columns = slice(lanes, lanes + LANES)

            def body(first):
                x = s.glu[pl.ds(first, window), columns]
                total = jnp.zeros((tile, LANES), F32)
                for shift in range(8):
                    moved = pltpu.roll(x, window - shift, 0) if shift else x
                    for k in range(n.taps):
                        at = PAD - half + k
                        if at % 8 == shift:
                            piece = moved[at - shift : at - shift + tile]
                            total = total + s.v_conv_taps[k : k + 1, columns] * piece
                s.cv[tp, pl.ds(first, tile), columns] = total.astype(BF16)

            each_tile(r, tile, body)
        cv.send(r)

    def mix_result(r):
        if r == 0:
            have("chan_gain", "chan_shift", "mix")
            ready(2)
        cv.wait(r)

        def body(first):
            rows = pl.ds(first, 32)
            total = jnp.zeros((32, 1), F32)
            square = jnp.zeros((32, 1), F32)
            for t in range(n.tps):
                v = s.cv[t, rows, :].astype(F32)
                total = total + jnp.sum(v, axis=-1, keepdims=True)
                square = square + jnp.sum(v * v, axis=-1, keepdims=True)
            mean = total / n.channels
            scale = lax.rsqrt(square / n.channels - mean * mean + 1e-05)
            for t in range(n.tps):
                columns = slice(t * n.own_channels, (t + 1) * n.own_channels)
                v = s.cv[t, rows, :].astype(F32)
                v = (v - mean) * scale * s.v_chan_gain[:, columns] + s.v_chan_shift[:, columns]
                s.hm[rows, columns] = (v * sigmoid(v)).astype(BF16)

        each_tile(r, 32, body)
        rows = rows_of(r)
        result = dot(s.hm[rows, :], s.wm[...])
        s.mx[tp, rows, :] = (s.tok[tp, rows, :].astype(F32) + result).astype(BF16)
        mx.send(r)

    def norm_two(r):
        have("mlp_gain")
        mx.wait(r)
        norm_rows(s.mx, s.v_mlp_gain, r)

    def mlp_in(c, r):
        first, width = n.mlp_cols[c]
        if r == 0:
            have("mgate", "mup", "gate_taps", "up_taps")
            ready(first_mlp + 2 * c)
            ready(first_mlp + 2 * c + 1)
        x = s.xn[rows_of(r), :]
        rows = pl.ds(EDGE + r * n.rows, n.rows)
        s.gp[rows, :width] = dot(x, s.wgate[:, first : first + width])
        s.up[rows, :width] = dot(x, s.wup[:, first : first + width])

    def mlp_act(c, r):
        first_column, width = n.mlp_cols[c]
        tile = 32
        window = tile + 2 * EDGE

        def filtered(values, taps, first, lanes, columns):
            x = values[pl.ds(first, window), lanes : lanes + LANES]
            low = pltpu.roll(x, 1, 0)[EDGE : EDGE + tile]
            high = pltpu.roll(x, window - 1, 0)[EDGE : EDGE + tile]
            middle = x[EDGE : EDGE + tile]
            return taps[0:1, columns] * low + taps[1:2, columns] * middle + taps[2:3, columns] * high

        def body(first):
            for lanes in range(0, width, LANES):
                columns = slice(first_column + lanes, first_column + lanes + LANES)
                gate = filtered(s.gp, s.v_gate_taps, first, lanes, columns)
                up = filtered(s.up, s.v_up_taps, first, lanes, columns)
                s.hidden[pl.ds(first, tile), columns] = (gate * sigmoid(gate) * up).astype(BF16)

        each_tile(r, tile, body)

    own_blocks = n.cols // LANES
    pending, settled = [], []

    def block_of(f, j):
        b = f * n.down_blocks + j
        owner = b // own_blocks
        return b, owner, owner % CORES

    def sib_index(b):
        return b // own_blocks // CORES * own_blocks + b % own_blocks

    def block_rows(r):
        return pl.ds(pl.multiple_of(r * n.block_rows, n.block_rows), n.block_rows)

    def to_sibling(b, r):
        return pltpu.make_async_remote_copy(
            src_ref=s.stage.at[b, block_rows(r)],
            dst_ref=s.sib_in.at[sib_index(b), block_rows(r)],
            send_sem=s.stage_send.at[0],
            recv_sem=s.sib_recv.at[sib_index(b), r],
            device_id={"tp": sibling},
            device_id_type=MESH,
        )

    def to_owner(b, r, owner, index):
        return pltpu.make_async_remote_copy(
            src_ref=s.stage.at[b, block_rows(r)],
            dst_ref=s.own_in.at[index, b % own_blocks, block_rows(r)],
            send_sem=s.stage_send.at[0],
            recv_sem=s.own_recv.at[index, b % own_blocks, r],
            device_id={"tp": owner},
            device_id_type=MESH,
        )

    def each_piece(body):
        def step(r, carry):
            body(r, block_rows(r))
            return carry

        lax.fori_loop(0, n.tokens // n.block_rows, step, 0)

    def collect(f, j, keep):
        b, owner, side = block_of(f, j)
        jump = (chip - owner // CORES + n.chips) % n.chips
        index = jnp.maximum(jump - 1, 0)

        @pl.when(jnp.logical_and(side == core, owner == tp))
        def _():
            def body(r, rows):
                to_sibling(b, r).wait_recv()
                s.total[b % own_blocks, rows, :] = s.kept[keep, rows, :] + s.sib_in[sib_index(b), rows, :].astype(F32)

            each_piece(body)

        @pl.when(jnp.logical_and(side == core, owner != tp))
        def _():
            def body(r, rows):
                to_sibling(b, r).wait_recv()
                both = s.kept[keep, rows, :] + s.sib_in[sib_index(b), rows, :].astype(F32)
                s.stage[b, rows, :] = both.astype(BF16)
                to_owner(b, r, owner, index).start()

            each_piece(body)

    def settle():
        if len(settled) < len(pending):
            collect(*pending[-1])
            settled.append(pending[-1])

    def block(f, j, step):
        last_columns = j == n.down_blocks - 1
        if step == 0:
            have("down")
        elif not last_columns:
            wait_y(first_down + j, f)
        b, owner, side = block_of(f, j)
        keep = len(pending) % 2
        columns = slice(j * LANES, (j + 1) * LANES)

        def body(r, rows):
            if step and last_columns:
                partial = s.early[step - 1, rows, :] + dot(s.hidden[rows, count:], s.wd[f, count:, columns])
            else:
                partial = dot(s.hidden[rows, :], s.wd[f, :, columns])

            @pl.when(side == core)
            def _():
                s.kept[keep, rows, :] = partial

            @pl.when(side != core)
            def _():
                s.stage[b, rows, :] = partial.astype(BF16)
                to_sibling(b, r).start()

        each_piece(body)
        settle()
        pending.append((f, j, keep))

    def early(f, j, step):
        settle()
        wait_y(first_down + j, f)
        columns = slice(j * LANES, (j + 1) * LANES)

        def body(r, rows):
            s.early[step - 1, rows, :] = dot(s.hidden[rows, :count], s.wd[f, :count, columns])

        each_piece(body)

    tasks = []

    def at(position, cost, work, *args):
        tasks.append((position, cost, work, args))

    def beats(count):
        return count / max(last, 1)

    for r in range(n.pieces):
        at(0.6 + 2.0 * (r / n.pieces) * 4 / 3, 0.2, tok.forward, r)
        at(1.0 + 2.0 * (r / n.pieces) * 4 / 3, 1.0, norm_one, r)
    for r in range(n.pieces):
        at(3.0, 1.5, mix_in, r)
    for r in range(n.pieces):
        at(3.6, 1.5, conv, r)
    for r in range(n.pieces):
        at(4.3 + 0.33 * r, 0.2, cv.forward, r)
        at(4.6 + 0.33 * r, 4.0, mix_result, r)
    for r in range(n.pieces):
        at(5.6 + 0.45 * r, 0.2, mx.forward, r)
        at(5.9 + 0.45 * r, 1.0, norm_two, r)
    for c in range(len(n.mlp_cols)):
        final = c == len(n.mlp_cols) - 1
        ready_at = first_mlp + 2 * (c + 1) + beats(n.mlp_lag - (1 if final else 0))
        for r in range(n.pieces):
            at(ready_at, 1.2, mlp_in, c, r)
        for r in range(n.pieces):
            at(ready_at, 0.6, mlp_act, c, r)
    own = 0
    for j in range(n.down_blocks):
        final = j == n.down_blocks - 1
        for step in range(1, n.shards):
            f = arrival(step)
            while own < n.down_blocks and own * OWN_AHEAD <= j * 2 * last + 2 * step - 2:
                at(0, 1.2, block, fs, own, 0)
                own += 1
            at(first_down + j + beats(step + n.down_lag), 1.2, early if final else block, f, j, step)
            if final:
                at(whole + beats(step), 1.2, block, f, j, step)
    assert own == n.down_blocks

    def run_tasks(now, budget):
        while tasks and tasks[0][0] <= now + 1e-6 and budget > 0:
            _, cost, work, args = tasks.pop(0)
            work(*args)
            budget -= cost

    peers = [("tp", (tp + jump) % n.tps) for jump in range(1, n.tps)]
    peers += [("grp", (group + jump) % n.groups) for jump in range(1, n.groups)]
    barrier = pltpu.get_barrier_semaphore()

    def greet(axis, index):
        pl.semaphore_signal(barrier, inc=1, device_id={axis: index}, device_id_type=MESH)

    for axis, index in peers:
        greet(axis, index)

    @pl.when(fs < last)
    def _():
        greet("fs", fs + 1)

    @pl.when(fs > 0)
    def _():
        greet("fs", fs - 1)

    ends = jnp.where(fs == 0, 1, 0) + jnp.where(fs == last, 1, 0)
    pl.semaphore_wait(barrier, len(peers) + 2 - ends)

    for r in range(n.pieces):
        tok.send(r)
        if r < LEAD:
            send_own(r)
    s.glu[:PAD, :] = jnp.zeros((PAD, n.own_channels), F32)
    s.glu[PAD + n.tokens :, :] = jnp.zeros((PAD, n.own_channels), F32)
    for ref in (s.gp, s.up):
        ref[:EDGE, :] = jnp.zeros((EDGE, ref.shape[1]), F32)
        ref[EDGE + n.tokens :, :] = jnp.zeros((EDGE, ref.shape[1]), F32)

    at_end = reach == 0

    def pump_own(i):
        pump(i, 1)

    for i in range(min(LEAD, n.chunks)):
        pl.when(at_end)(functools.partial(pump_own, i))
    for i in range(n.chunks):
        pl.when(jnp.logical_not(at_end))(functools.partial(pump_own, i))
        run_tasks(i + 1 / last, BUDGET)
        for step in range(2, n.shards):
            pump(i, step)
            if step < last:
                run_tasks(i + step / last, BUDGET)
        if i + LEAD < n.chunks:
            send_own(i + LEAD)
            pl.when(at_end)(functools.partial(pump_own, i + LEAD))
        run_tasks(i + 1.0, BUDGET)
    run_tasks(1e9, 1e9)
    settle()

    have("final_gain")

    def sum_up(first):
        rows = pl.ds(first, LANES)
        squares = jnp.zeros((LANES, LANES), F32)
        for j in range(own_blocks):
            columns = slice(j * LANES, (j + 1) * LANES)
            v = s.total[j, rows, :] + s.mx[tp, rows, columns].astype(F32)
            for jump in range(1, n.chips):
                v = v + s.own_in[jump - 1, j, rows, :].astype(F32)
            s.total[j, rows, :] = v
            squares = squares + v * v
        across = jnp.sum(jnp.transpose(squares), axis=0, keepdims=True)
        s.stats[tp, :, rows] = jnp.broadcast_to(across, (8, LANES))

    def sum_piece(r, rows):
        for jump in range(1, n.chips):
            for j in range(own_blocks):
                to_owner(j, r, sibling, jump - 1).wait_recv()
        for first in range(0, n.block_rows, LANES):
            sum_up(pl.multiple_of(r * n.block_rows + first, LANES))

    def each_block(body):
        def step(q, carry):
            body(pl.multiple_of(q * LANES, LANES))
            return carry

        lax.fori_loop(0, n.tokens // LANES, step, 0)

    each_piece(sum_piece)

    def stats_copy(refs, jump):
        return pltpu.make_async_remote_copy(
            src_ref=refs,
            dst_ref=refs,
            send_sem=s.stats_send.at[0],
            recv_sem=s.stats_recv.at[0],
            device_id={"tp": (tp + jump) % n.tps},
            device_id_type=MESH,
        )

    for jump in range(1, n.tps):
        stats_copy(s.stats.at[tp], jump).start()
    drain()
    for gather in (tok, cv, mx):
        gather.drain()
    refs = s.stage.at[pl.ds(0, n.shards * n.down_blocks - own_blocks)]
    pltpu.make_async_remote_copy(
        src_ref=refs,
        dst_ref=refs,
        send_sem=s.stage_send.at[0],
        recv_sem=s.stats_recv.at[0],
        device_id={"tp": sibling},
        device_id_type=MESH,
    ).wait_send()
    all_stats = s.stats.at[pl.ds(0, n.tps - 1)]
    stats_copy(all_stats, 1).wait_recv()

    def finish(first):
        rows = pl.ds(first, LANES)
        across = s.stats[0, 0:1, rows]
        for t in range(1, n.tps):
            across = across + s.stats[t, 0:1, rows]
        square = jnp.transpose(jnp.broadcast_to(across, (LANES, LANES)))
        scale = lax.rsqrt(square / n.width + 1e-06)
        for j in range(own_blocks):
            columns = slice(j * LANES, (j + 1) * LANES)
            s.result[rows, columns] = (s.total[j, rows, :] * scale * s.v_final_gain[:, columns]).astype(BF16)

        pltpu.make_async_copy(s.result.at[rows, :], out.at[rows, :], s.out_sem.at[0]).start()

    each_block(finish)
    pltpu.make_async_copy(s.result, out, s.out_sem.at[0]).wait()
    stats_copy(all_stats, 1).wait_send()


def wide(array, axis):
    extra = -array.shape[axis] % LANES
    if not extra:
        return array
    return jnp.pad(array, [(0, extra if k == axis else 0) for k in range(array.ndim)])


INPUTS = (
    "tokens",
    "mix_gain",
    "value",
    "gate",
    "conv_taps",
    "chan_gain",
    "chan_shift",
    "mix",
    "mlp_gain",
    "mgate",
    "mup",
    "gate_taps",
    "up_taps",
    "down",
    "final_gain",
)
SMALL = (
    "mix_gain",
    "conv_taps",
    "chan_gain",
    "chan_shift",
    "mlp_gain",
    "gate_taps",
    "up_taps",
    "final_gain",
)


def local(*values):
    a = dict(zip(INPUTS, values))
    for name in ("mix_gain", "chan_gain", "chan_shift", "mlp_gain", "final_gain"):
        a[name] = a[name][None]
    for name in ("mgate", "mup", "gate_taps", "up_taps"):
        a[name] = wide(a[name], 1)
    a["down"] = wide(a["down"], 0)
    tps, shards, groups = lax.axis_size("tp"), lax.axis_size("fs"), lax.axis_size("grp")
    chips = tps // CORES
    tokens, cols = a["tokens"].shape
    depth, own_channels = a["value"].shape
    hidden = a["mgate"].shape[1]
    mlp_cols = column_chunks(hidden, 3 * LANES)
    down_blocks = a["down"].shape[1] // LANES
    rows = min(256, tokens)
    pieces = tokens // rows
    block_rows = min(BLOCK_ROWS, tokens)
    chunks = 4 + 2 * len(mlp_cols) + down_blocks
    whole_rows = hidden * WHOLE // 8 // LANES * LANES
    width, channels = cols * tps, own_channels * tps
    blocks = shards * down_blocks
    own_blocks = cols // LANES
    edge = tokens + 2 * EDGE
    vmem, dma = pltpu.VMEM, pltpu.SemaphoreType.DMA
    scratch = {
        "tok": vmem((tps, tokens, cols), BF16),
        "cv": vmem((tps, tokens, own_channels), BF16),
        "mx": vmem((tps, tokens, cols), BF16),
        "xn": vmem((tokens, width), BF16),
        "hm": vmem((tokens, channels), BF16),
        "glu": vmem((tokens + 2 * PAD, own_channels), F32),
        "gp": vmem((edge, mlp_cols[0][1]), F32),
        "up": vmem((edge, mlp_cols[0][1]), F32),
        "hidden": vmem((tokens, hidden), BF16),
        "wv": vmem((width, own_channels), BF16),
        "wg": vmem((width, own_channels), BF16),
        "wm": vmem((channels, cols), BF16),
        "wgate": vmem((width, hidden), BF16),
        "wup": vmem((width, hidden), BF16),
        "wd": vmem((shards,) + a["down"].shape, BF16),
        "early": vmem((shards - 1, tokens, LANES), F32),
        "kept": vmem((2, tokens, LANES), F32),
        "stage": vmem((blocks, tokens, LANES), BF16),
        "sib_in": vmem((blocks // CORES, tokens, LANES), BF16),
        "own_in": vmem((chips - 1, own_blocks, tokens, LANES), BF16),
        "total": vmem((own_blocks, tokens, LANES), F32),
        "stats": vmem((tps, 8, tokens), F32),
        "result": vmem((tokens, cols), BF16),
        "out_sem": dma((1,)),
        "local_sem": dma((7 + len(SMALL),)),
        "z_recv": dma((chunks, shards)),
        "up_send": dma((8,)),
        "down_send": dma((8,)),
        "y_send": dma((groups - 1, 8)),
        "y_recv": dma((groups - 1, chunks - down_blocks - 1)),
        "y_down": dma((groups - 1, down_blocks, shards)),
        "gather_send": dma((3,)),
        "gather_chip": dma((3, chips - 1, pieces)),
        "gather_core": dma((3, pieces)),
        "stage_send": dma((1,)),
        "sib_recv": dma((blocks // CORES, tokens // block_rows)),
        "own_recv": dma((chips - 1, own_blocks, tokens // block_rows)),
        "stats_send": dma((1,)),
        "stats_recv": dma((1,)),
    }
    for name in SMALL:
        scratch["v_" + name] = vmem(a[name].shape, F32)
    n = SimpleNamespace(
        inputs=INPUTS,
        small=SMALL,
        scratch=tuple(scratch),
        tps=tps,
        shards=shards,
        groups=groups,
        chips=chips,
        tokens=tokens,
        rows=rows,
        pieces=pieces,
        block_rows=block_rows,
        cols=cols,
        width=width,
        channels=channels,
        own_channels=own_channels,
        depth=depth,
        mix_depth=a["mix"].shape[0],
        hidden=hidden,
        mlp_cols=mlp_cols,
        down_blocks=down_blocks,
        whole_rows=whole_rows,
        mlp_lag=MLP_LAG,
        down_lag=DOWN_LAG,
        chunks=chunks,
        taps=a["conv_taps"].shape[0],
    )
    return pl.pallas_call(
        functools.partial(layer_kernel, n),
        out_shape=jax.ShapeDtypeStruct((tokens, cols), BF16),
        in_specs=[pl.BlockSpec(memory_space=pl.ANY)] * len(INPUTS),
        out_specs=pl.BlockSpec(memory_space=pl.ANY),
        scratch_shapes=list(scratch.values()),
        compiler_params=pltpu.CompilerParams(
            collective_id=0, has_side_effects=True, vmem_limit_bytes=GRANT
        ),
        name="layer",
    )(*[a[name] for name in INPUTS])


def solution(mesh):
    return jax.shard_map(
        local,
        mesh=mesh,
        in_specs=(
            P(("grp", "fs"), "tp"),
            P(),
            P("fs", "tp"),
            P("fs", "tp"),
            P(None, "tp"),
            P(),
            P(),
            P("fs", "tp"),
            P(),
            P("fs", "tp"),
            P("fs", "tp"),
            P(None, "tp"),
            P(None, "tp"),
            P("tp", "fs"),
            P("tp"),
        ),
        out_specs=P(("grp", "fs"), "tp"),
        check_vma=False,
    )
```

```python
import functools
from types import SimpleNamespace

import jax
import jax.numpy as jnp
from jax import lax
from jax.experimental import pallas as pl
from jax.experimental.pallas import tpu as pltpu
from jax.sharding import PartitionSpec as P

MESH = pl.DeviceIdType.MESH
F32, BF16 = jnp.float32, jnp.bfloat16
LANES = 128
CORES = 2
LEAD = 2
BLOCK_ROWS = 512
GRANT = 67043328
WHOLE = 4
MLP_LAG = 4
DOWN_LAG = 3
OWN_AHEAD = 5
PAD = 16
EDGE = 8
BUDGET = 3.4


def column_chunks(width, most):
    return [(first, min(most, width - first)) for first in range(0, width, most)]


def sigmoid(value):
    return 1.0 / (1.0 + jnp.exp(-value))


def layer_kernel(n, *refs):
    arrays = SimpleNamespace(**dict(zip(n.inputs, refs)))
    out = refs[len(n.inputs)]
    s = SimpleNamespace(**dict(zip(n.scratch, refs[len(n.inputs) + 1 :])))

    group, fs, tp = lax.axis_index("grp"), lax.axis_index("fs"), lax.axis_index("tp")
    chip, core = tp // CORES, tp % CORES
    sibling = tp + 1 - 2 * core

    def chip_at(jump):
        return (chip + jump + n.chips) % n.chips

    def rows_of(r):
        return pl.ds(r * n.rows, n.rows)

    local = {}

    def load(name, src, dst):
        index = len(local)
        local[name] = pltpu.make_async_copy(src, dst, s.local_sem.at[index])
        local[name].start()

    loaded = set()

    def have(*names):
        for name in names:
            if name not in loaded:
                loaded.add(name)
                local[name].wait()

    def own_rows(dst, count):
        return dst.at[pl.ds(pl.multiple_of(fs * count, count), count), :]

    load("tokens", arrays.tokens, s.tok.at[tp])
    for name in n.small:
        load(name, getattr(arrays, name), getattr(s, "v_" + name))
    load("value", arrays.value, own_rows(s.wv, n.depth))
    load("gate", arrays.gate, own_rows(s.wg, n.depth))
    load("mix", arrays.mix, own_rows(s.wm, n.mix_depth))
    load("mgate", arrays.mgate, own_rows(s.wgate, n.depth))
    load("mup", arrays.mup, own_rows(s.wup, n.depth))
    load("down", arrays.down, s.wd.at[fs])

    chunks = [
        (arrays.value, s.wv, 0, n.depth, 0, n.own_channels),
        (arrays.gate, s.wg, 0, n.depth, 0, n.own_channels),
        (arrays.mix, s.wm, 0, n.mix_depth, 0, n.cols),
    ]
    first_mlp = len(chunks)
    for first, width in n.mlp_cols:
        chunks.append((arrays.mgate, s.wgate, 0, n.depth, first, width))
        chunks.append((arrays.mup, s.wup, 0, n.depth, first, width))
    first_down = len(chunks)
    for j in range(n.down_blocks):
        count = n.hidden - (n.whole_rows if j == n.down_blocks - 1 else 0)
        chunks.append((arrays.down, s.wd, 0, count, j * LANES, LANES))
    whole = len(chunks)
    chunks.append((arrays.down, s.wd, count, n.whole_rows, j * LANES, LANES))
    assert len(chunks) == n.chunks
    kinds = [0, 1, 2] + [3 + i % 2 for i in range(first_down - first_mlp)]
    kinds += [5] * (n.down_blocks - 1) + [6, 7]

    def part_rows(i, part):
        row, count = chunks[i][2:4]
        if i == whole:
            return row, count
        half = count // n.groups
        return pl.multiple_of(row + part * half, half), half

    def slot(i, f, part):
        _, dst, _, _, first, width = chunks[i]
        row, half = part_rows(i, part)
        columns = pl.ds(first, width)
        if i >= first_down:
            return dst.at[f, pl.ds(row, half), columns]
        return dst.at[pl.ds(pl.multiple_of(f * chunks[i][3] + row, half), half), columns]

    def z_copy(i, f, to, sems, own=False):
        src = slot(i, f, group)
        if own:
            source, _, _, _, first, width = chunks[i]
            row, half = part_rows(i, group)
            src = source.at[pl.ds(row, half), pl.ds(first, width)]
        return pltpu.make_async_remote_copy(
            src_ref=src,
            dst_ref=slot(i, f, group),
            send_sem=sems.at[kinds[i]],
            recv_sem=s.z_recv.at[i, f],
            device_id={"fs": to},
            device_id_type=MESH,
        )

    def y_copy(i, f, jump, part, refs=None):
        refs = slot(i, f, part) if refs is None else refs
        down = i >= first_down
        recv_sem = s.y_down.at[jump - 1, i - first_down, f] if down else s.y_recv.at[jump - 1, i]
        return pltpu.make_async_remote_copy(
            src_ref=refs,
            dst_ref=refs,
            send_sem=s.y_send.at[jump - 1, kinds[i]],
            recv_sem=recv_sem,
            device_id={"grp": (group + jump) % n.groups},
            device_id_type=MESH,
        )

    last = n.shards - 1
    reach = jnp.minimum(fs, last - fs)

    def arrival(step):
        near = fs - (step + 1) // 2 if step % 2 else fs + (step + 1) // 2
        distance = step - reach
        far = jnp.where(fs > last - fs, fs - distance, fs + distance)
        return jnp.where(step <= 2 * reach, near, far)

    def send_own(i):
        @pl.when(fs < last)
        def _():
            z_copy(i, fs, fs + 1, s.up_send, own=True).start()

        @pl.when(fs > 0)
        def _():
            z_copy(i, fs, fs - 1, s.down_send, own=True).start()

    def pump(i, step):
        f = arrival(step)
        z_copy(i, f, fs, s.up_send).wait_recv()

        @pl.when(jnp.logical_and(f < fs, fs < last))
        def _():
            z_copy(i, f, fs + 1, s.up_send).start()

        @pl.when(jnp.logical_and(f > fs, fs > 0))
        def _():
            z_copy(i, f, fs - 1, s.down_send).start()

        for jump in range(1, n.groups if i != whole else 1):
            y_copy(i, f, jump, group).start()

    def wait_y(i, f):
        for jump in range(1, n.groups):
            y_copy(i, f, jump, (group - jump + n.groups) % n.groups).wait_recv()

    def ready(i):
        _, dst, _, depth, first, width = chunks[i]
        refs = dst.at[pl.ds(0, last * (depth // n.groups)), pl.ds(first, width)]
        for jump in range(1, n.groups):
            y_copy(i, fs, jump, group, refs).wait_recv()

    def sent(kind, count):
        i = kinds.index(kind)
        _, dst, _, depth, _, _ = chunks[i]
        half = depth if kind == 7 else depth // n.groups
        if kind < 5:
            return i, dst.at[pl.ds(0, count * half), :]
        columns = (n.down_blocks - 1 if kind == 5 else 1) * LANES
        return i, dst.at[pl.ds(0, count), pl.ds(0, half), pl.ds(0, columns)]

    def drain():
        def wait(sems, to, count, kind):
            i, refs = sent(kind, count)
            pltpu.make_async_remote_copy(
                src_ref=refs,
                dst_ref=refs,
                send_sem=sems.at[kind],
                recv_sem=s.z_recv.at[0, 0],
                device_id={"fs": to},
                device_id_type=MESH,
            ).wait_send()

        used = sorted(set(kinds))
        for count in range(1, n.shards):

            @pl.when(fs + 1 == count)
            def _():
                for kind in used:
                    wait(s.up_send, fs + 1, count, kind)

            @pl.when(last - fs + 1 == count)
            def _():
                for kind in used:
                    wait(s.down_send, fs - 1, count, kind)

        for kind in used[:-1]:
            i, refs = sent(kind, last)
            for jump in range(1, n.groups):
                y_copy(i, fs, jump, group, refs).wait_send()

    class Gather:
        def __init__(self, blocks, kind, own=None):
            self.blocks, self.kind, self.own = blocks, kind, own

        def copy(self, block, r, to, jump, src=None):
            dst = self.blocks.at[block, rows_of(r), :]
            sems = s.gather_chip.at[self.kind, jump - 1, r] if jump else s.gather_core.at[self.kind, r]
            return pltpu.make_async_remote_copy(
                src_ref=dst if src is None else src,
                dst_ref=dst,
                send_sem=s.gather_send.at[self.kind],
                recv_sem=sems,
                device_id={"tp": to},
                device_id_type=MESH,
            )

        def send(self, r):
            src = None if self.own is None else self.own.at[rows_of(r), :]
            for jump in range(1, n.chips):
                self.copy(tp, r, chip_at(jump) * CORES + core, jump, src).start()
            self.copy(tp, r, sibling, 0, src).start()

        def forward(self, r):
            for jump in range(1, n.chips):
                block = chip_at(-jump) * CORES + core
                self.copy(block, r, sibling, jump).wait_recv()
                self.copy(block, r, sibling, 0).start()

        def wait(self, r):
            refs = self.blocks.at[pl.ds(0, n.chips), rows_of(r), :]
            pltpu.make_async_remote_copy(
                src_ref=refs,
                dst_ref=refs,
                send_sem=s.gather_send.at[self.kind],
                recv_sem=s.gather_core.at[self.kind, r],
                device_id={"tp": sibling},
                device_id_type=MESH,
            ).wait_recv()

        def drain(self):
            refs = self.blocks.at[pl.ds(0, 2 * n.chips - 1)]
            pltpu.make_async_remote_copy(
                src_ref=refs,
                dst_ref=refs,
                send_sem=s.gather_send.at[self.kind],
                recv_sem=s.gather_core.at[self.kind, 0],
                device_id={"tp": sibling},
                device_id_type=MESH,
            ).wait_send()

    tok = Gather(s.tok, 0, arrays.tokens)
    cv = Gather(s.cv, 1)
    mx = Gather(s.mx, 2)

    def each_tile(r, size, body):
        def step(q, carry):
            body(pl.multiple_of(r * n.rows + q * size, size))
            return carry

        lax.fori_loop(0, n.rows // size, step, 0)

    def norm_rows(blocks, gain, r):
        def body(first):
            rows = pl.ds(first, 32)
            total = jnp.zeros((32, 1), F32)
            for t in range(n.tps):
                v = blocks[t, rows, :].astype(F32)
                total = total + jnp.sum(v * v, axis=-1, keepdims=True)
            scale = lax.rsqrt(total / n.width + 1e-06)
            for t in range(n.tps):
                columns = slice(t * n.cols, (t + 1) * n.cols)
                v = blocks[t, rows, :].astype(F32)
                s.xn[rows, columns] = (v * scale * gain[:, columns]).astype(BF16)

        each_tile(r, 32, body)

    def dot(a, b):
        return jnp.dot(a, b, preferred_element_type=F32)

    def norm_one(r):
        have("tokens", "mix_gain")
        tok.wait(r)
        norm_rows(s.tok, s.v_mix_gain, r)

    def mix_in(r):
        if r == 0:
            have("value", "gate", "conv_taps")
            ready(0)
            ready(1)
        x = s.xn[rows_of(r), :]
        value = dot(x, s.wv[...])
        gate = dot(x, s.wg[...])
        s.glu[pl.ds(PAD + r * n.rows, n.rows), :] = value * sigmoid(gate)

    def conv(r):
        tile, half = 64, (n.taps - 1) // 2
        window = tile + 2 * PAD
        for lanes in range(0, n.own_channels, LANES):
            columns = slice(lanes, lanes + LANES)

            def body(first):
                x = s.glu[pl.ds(first, window), columns]
                total = jnp.zeros((tile, LANES), F32)
                for shift in range(8):
                    moved = pltpu.roll(x, window - shift, 0) if shift else x
                    for k in range(n.taps):
                        at = PAD - half + k
                        if at % 8 == shift:
                            piece = moved[at - shift : at - shift + tile]
                            total = total + s.v_conv_taps[k : k + 1, columns] * piece
                s.cv[tp, pl.ds(first, tile), columns] = total.astype(BF16)

            each_tile(r, tile, body)
        cv.send(r)

    def mix_result(r):
        if r == 0:
            have("chan_gain", "chan_shift", "mix")
            ready(2)
        cv.wait(r)

        def body(first):
            rows = pl.ds(first, 32)
            total = jnp.zeros((32, 1), F32)
            square = jnp.zeros((32, 1), F32)
            for t in range(n.tps):
                v = s.cv[t, rows, :].astype(F32)
                total = total + jnp.sum(v, axis=-1, keepdims=True)
                square = square + jnp.sum(v * v, axis=-1, keepdims=True)
            mean = total / n.channels
            scale = lax.rsqrt(square / n.channels - mean * mean + 1e-05)
            for t in range(n.tps):
                columns = slice(t * n.own_channels, (t + 1) * n.own_channels)
                v = s.cv[t, rows, :].astype(F32)
                v = (v - mean) * scale * s.v_chan_gain[:, columns] + s.v_chan_shift[:, columns]
                s.hm[rows, columns] = (v * sigmoid(v)).astype(BF16)

        each_tile(r, 32, body)
        rows = rows_of(r)
        result = dot(s.hm[rows, :], s.wm[...])
        s.mx[tp, rows, :] = (s.tok[tp, rows, :].astype(F32) + result).astype(BF16)
        mx.send(r)

    def norm_two(r):
        have("mlp_gain")
        mx.wait(r)
        norm_rows(s.mx, s.v_mlp_gain, r)

    def mlp_in(c, r):
        first, width = n.mlp_cols[c]
        if r == 0:
            have("mgate", "mup", "gate_taps", "up_taps")
            ready(first_mlp + 2 * c)
            ready(first_mlp + 2 * c + 1)
        x = s.xn[rows_of(r), :]
        rows = pl.ds(EDGE + r * n.rows, n.rows)
        s.gp[rows, :width] = dot(x, s.wgate[:, first : first + width])
        s.up[rows, :width] = dot(x, s.wup[:, first : first + width])

    def mlp_act(c, r):
        first_column, width = n.mlp_cols[c]
        tile = 32
        window = tile + 2 * EDGE

        def filtered(values, taps, first, lanes, columns):
            x = values[pl.ds(first, window), lanes : lanes + LANES]
            low = pltpu.roll(x, 1, 0)[EDGE : EDGE + tile]
            high = pltpu.roll(x, window - 1, 0)[EDGE : EDGE + tile]
            middle = x[EDGE : EDGE + tile]
            return taps[0:1, columns] * low + taps[1:2, columns] * middle + taps[2:3, columns] * high

        def body(first):
            for lanes in range(0, width, LANES):
                columns = slice(first_column + lanes, first_column + lanes + LANES)
                gate = filtered(s.gp, s.v_gate_taps, first, lanes, columns)
                up = filtered(s.up, s.v_up_taps, first, lanes, columns)
                s.hidden[pl.ds(first, tile), columns] = (gate * sigmoid(gate) * up).astype(BF16)

        each_tile(r, tile, body)

    own_blocks = n.cols // LANES
    pending, settled = [], []

    def block_of(f, j):
        b = f * n.down_blocks + j
        owner = b // own_blocks
        return b, owner, owner % CORES

    def sib_index(b):
        return b // own_blocks // CORES * own_blocks + b % own_blocks

    def block_rows(r):
        return pl.ds(pl.multiple_of(r * n.block_rows, n.block_rows), n.block_rows)

    def to_sibling(b, r):
        return pltpu.make_async_remote_copy(
            src_ref=s.stage.at[b, block_rows(r)],
            dst_ref=s.sib_in.at[sib_index(b), block_rows(r)],
            send_sem=s.stage_send.at[0],
            recv_sem=s.sib_recv.at[sib_index(b), r],
            device_id={"tp": sibling},
            device_id_type=MESH,
        )

    def to_owner(b, r, owner, index):
        return pltpu.make_async_remote_copy(
            src_ref=s.stage.at[b, block_rows(r)],
            dst_ref=s.own_in.at[index, b % own_blocks, block_rows(r)],
            send_sem=s.stage_send.at[0],
            recv_sem=s.own_recv.at[index, b % own_blocks, r],
            device_id={"tp": owner},
            device_id_type=MESH,
        )

    def each_piece(body):
        def step(r, carry):
            body(r, block_rows(r))
            return carry

        lax.fori_loop(0, n.tokens // n.block_rows, step, 0)

    def collect(f, j, keep):
        b, owner, side = block_of(f, j)
        jump = (chip - owner // CORES + n.chips) % n.chips
        index = jnp.maximum(jump - 1, 0)

        @pl.when(jnp.logical_and(side == core, owner == tp))
        def _():
            def body(r, rows):
                to_sibling(b, r).wait_recv()
                s.total[b % own_blocks, rows, :] = s.kept[keep, rows, :] + s.sib_in[sib_index(b), rows, :].astype(F32)

            each_piece(body)

        @pl.when(jnp.logical_and(side == core, owner != tp))
        def _():
            def body(r, rows):
                to_sibling(b, r).wait_recv()
                both = s.kept[keep, rows, :] + s.sib_in[sib_index(b), rows, :].astype(F32)
                s.stage[b, rows, :] = both.astype(BF16)
                to_owner(b, r, owner, index).start()

            each_piece(body)

    def settle():
        if len(settled) < len(pending):
            collect(*pending[-1])
            settled.append(pending[-1])

    def block(f, j, step):
        last_columns = j == n.down_blocks - 1
        if step == 0:
            have("down")
        elif not last_columns:
            wait_y(first_down + j, f)
        b, owner, side = block_of(f, j)
        keep = len(pending) % 2
        columns = slice(j * LANES, (j + 1) * LANES)

        def body(r, rows):
            if step and last_columns:
                partial = s.early[step - 1, rows, :] + dot(s.hidden[rows, count:], s.wd[f, count:, columns])
            else:
                partial = dot(s.hidden[rows, :], s.wd[f, :, columns])

            @pl.when(side == core)
            def _():
                s.kept[keep, rows, :] = partial

            @pl.when(side != core)
            def _():
                s.stage[b, rows, :] = partial.astype(BF16)
                to_sibling(b, r).start()

        each_piece(body)
        settle()
        pending.append((f, j, keep))

    def early(f, j, step):
        settle()
        wait_y(first_down + j, f)
        columns = slice(j * LANES, (j + 1) * LANES)

        def body(r, rows):
            s.early[step - 1, rows, :] = dot(s.hidden[rows, :count], s.wd[f, :count, columns])

        each_piece(body)

    tasks = []

    def at(position, cost, work, *args):
        tasks.append((position, cost, work, args))

    def beats(count):
        return count / max(last, 1)

    for r in range(n.pieces):
        at(0.6 + 2.0 * (r / n.pieces) * 4 / 3, 0.2, tok.forward, r)
        at(1.0 + 2.0 * (r / n.pieces) * 4 / 3, 1.0, norm_one, r)
    for r in range(n.pieces):
        at(3.0, 1.5, mix_in, r)
    for r in range(n.pieces):
        at(3.6, 1.5, conv, r)
    for r in range(n.pieces):
        at(4.3 + 0.33 * r, 0.2, cv.forward, r)
        at(4.6 + 0.33 * r, 4.0, mix_result, r)
    for r in range(n.pieces):
        at(5.6 + 0.45 * r, 0.2, mx.forward, r)
        at(5.9 + 0.45 * r, 1.0, norm_two, r)
    for c in range(len(n.mlp_cols)):
        final = c == len(n.mlp_cols) - 1
        ready_at = first_mlp + 2 * (c + 1) + beats(n.mlp_lag - (1 if final else 0))
        for r in range(n.pieces):
            at(ready_at, 1.2, mlp_in, c, r)
        for r in range(n.pieces):
            at(ready_at, 0.6, mlp_act, c, r)
    own = 0
    for j in range(n.down_blocks):
        final = j == n.down_blocks - 1
        for step in range(1, n.shards):
            f = arrival(step)
            while own < n.down_blocks and own * OWN_AHEAD <= j * 2 * last + 2 * step - 2:
                at(0, 1.2, block, fs, own, 0)
                own += 1
            at(first_down + j + beats(step + n.down_lag), 1.2, early if final else block, f, j, step)
            if final:
                at(whole + beats(step), 1.2, block, f, j, step)
    assert own == n.down_blocks

    def run_tasks(now, budget):
        while tasks and tasks[0][0] <= now + 1e-6 and budget > 0:
            _, cost, work, args = tasks.pop(0)
            work(*args)
            budget -= cost

    peers = [("tp", (tp + jump) % n.tps) for jump in range(1, n.tps)]
    peers += [("grp", (group + jump) % n.groups) for jump in range(1, n.groups)]
    barrier = pltpu.get_barrier_semaphore()

    def greet(axis, index):
        pl.semaphore_signal(barrier, inc=1, device_id={axis: index}, device_id_type=MESH)

    for axis, index in peers:
        greet(axis, index)

    @pl.when(fs < last)
    def _():
        greet("fs", fs + 1)

    @pl.when(fs > 0)
    def _():
        greet("fs", fs - 1)

    ends = jnp.where(fs == 0, 1, 0) + jnp.where(fs == last, 1, 0)
    pl.semaphore_wait(barrier, len(peers) + 2 - ends)

    for r in range(n.pieces):
        tok.send(r)
        if r < LEAD:
            send_own(r)
    s.glu[:PAD, :] = jnp.zeros((PAD, n.own_channels), F32)
    s.glu[PAD + n.tokens :, :] = jnp.zeros((PAD, n.own_channels), F32)
    for ref in (s.gp, s.up):
        ref[:EDGE, :] = jnp.zeros((EDGE, ref.shape[1]), F32)
        ref[EDGE + n.tokens :, :] = jnp.zeros((EDGE, ref.shape[1]), F32)

    at_end = reach == 0

    def pump_own(i):
        pump(i, 1)

    for i in range(min(LEAD, n.chunks)):
        pl.when(at_end)(functools.partial(pump_own, i))
    for i in range(n.chunks):
        pl.when(jnp.logical_not(at_end))(functools.partial(pump_own, i))
        run_tasks(i + 1 / last, BUDGET)
        for step in range(2, n.shards):
            pump(i, step)
            if step < last:
                run_tasks(i + step / last, BUDGET)
        if i + LEAD < n.chunks:
            send_own(i + LEAD)
        run_tasks(i + 1.0, BUDGET)
        if i + LEAD < n.chunks:
            pl.when(at_end)(functools.partial(pump_own, i + LEAD))
    run_tasks(1e9, 1e9)
    settle()

    have("final_gain")

    def sum_up(first):
        rows = pl.ds(first, LANES)
        squares = jnp.zeros((LANES, LANES), F32)
        for j in range(own_blocks):
            columns = slice(j * LANES, (j + 1) * LANES)
            v = s.total[j, rows, :] + s.mx[tp, rows, columns].astype(F32)
            for jump in range(1, n.chips):
                v = v + s.own_in[jump - 1, j, rows, :].astype(F32)
            s.total[j, rows, :] = v
            squares = squares + v * v
        across = jnp.sum(jnp.transpose(squares), axis=0, keepdims=True)
        s.stats[tp, :, rows] = jnp.broadcast_to(across, (8, LANES))

    def sum_piece(r, rows):
        for jump in range(1, n.chips):
            for j in range(own_blocks):
                to_owner(j, r, sibling, jump - 1).wait_recv()
        for first in range(0, n.block_rows, LANES):
            sum_up(pl.multiple_of(r * n.block_rows + first, LANES))

    def each_block(body):
        def step(q, carry):
            body(pl.multiple_of(q * LANES, LANES))
            return carry

        lax.fori_loop(0, n.tokens // LANES, step, 0)

    each_piece(sum_piece)

    def stats_copy(refs, jump):
        return pltpu.make_async_remote_copy(
            src_ref=refs,
            dst_ref=refs,
            send_sem=s.stats_send.at[0],
            recv_sem=s.stats_recv.at[0],
            device_id={"tp": (tp + jump) % n.tps},
            device_id_type=MESH,
        )

    for jump in range(1, n.tps):
        stats_copy(s.stats.at[tp], jump).start()
    drain()
    for gather in (tok, cv, mx):
        gather.drain()
    refs = s.stage.at[pl.ds(0, n.shards * n.down_blocks - own_blocks)]
    pltpu.make_async_remote_copy(
        src_ref=refs,
        dst_ref=refs,
        send_sem=s.stage_send.at[0],
        recv_sem=s.stats_recv.at[0],
        device_id={"tp": sibling},
        device_id_type=MESH,
    ).wait_send()
    all_stats = s.stats.at[pl.ds(0, n.tps - 1)]
    stats_copy(all_stats, 1).wait_recv()

    def finish(first):
        rows = pl.ds(first, LANES)
        across = s.stats[0, 0:1, rows]
        for t in range(1, n.tps):
            across = across + s.stats[t, 0:1, rows]
        square = jnp.transpose(jnp.broadcast_to(across, (LANES, LANES)))
        scale = lax.rsqrt(square / n.width + 1e-06)
        for j in range(own_blocks):
            columns = slice(j * LANES, (j + 1) * LANES)
            s.result[rows, columns] = (s.total[j, rows, :] * scale * s.v_final_gain[:, columns]).astype(BF16)

        pltpu.make_async_copy(s.result.at[rows, :], out.at[rows, :], s.out_sem.at[0]).start()

    each_block(finish)
    pltpu.make_async_copy(s.result, out, s.out_sem.at[0]).wait()
    stats_copy(all_stats, 1).wait_send()


def wide(array, axis):
    extra = -array.shape[axis] % LANES
    if not extra:
        return array
    return jnp.pad(array, [(0, extra if k == axis else 0) for k in range(array.ndim)])


INPUTS = (
    "tokens",
    "mix_gain",
    "value",
    "gate",
    "conv_taps",
    "chan_gain",
    "chan_shift",
    "mix",
    "mlp_gain",
    "mgate",
    "mup",
    "gate_taps",
    "up_taps",
    "down",
    "final_gain",
)
SMALL = (
    "mix_gain",
    "conv_taps",
    "chan_gain",
    "chan_shift",
    "mlp_gain",
    "gate_taps",
    "up_taps",
    "final_gain",
)


def local(*values):
    a = dict(zip(INPUTS, values))
    for name in ("mix_gain", "chan_gain", "chan_shift", "mlp_gain", "final_gain"):
        a[name] = a[name][None]
    for name in ("mgate", "mup", "gate_taps", "up_taps"):
        a[name] = wide(a[name], 1)
    a["down"] = wide(a["down"], 0)
    tps, shards, groups = lax.axis_size("tp"), lax.axis_size("fs"), lax.axis_size("grp")
    chips = tps // CORES
    tokens, cols = a["tokens"].shape
    depth, own_channels = a["value"].shape
    hidden = a["mgate"].shape[1]
    mlp_cols = column_chunks(hidden, 3 * LANES)
    down_blocks = a["down"].shape[1] // LANES
    rows = min(256, tokens)
    pieces = tokens // rows
    block_rows = min(BLOCK_ROWS, tokens)
    chunks = 4 + 2 * len(mlp_cols) + down_blocks
    whole_rows = hidden * WHOLE // 8 // LANES * LANES
    width, channels = cols * tps, own_channels * tps
    blocks = shards * down_blocks
    own_blocks = cols // LANES
    edge = tokens + 2 * EDGE
    vmem, dma = pltpu.VMEM, pltpu.SemaphoreType.DMA
    scratch = {
        "tok": vmem((tps, tokens, cols), BF16),
        "cv": vmem((tps, tokens, own_channels), BF16),
        "mx": vmem((tps, tokens, cols), BF16),
        "xn": vmem((tokens, width), BF16),
        "hm": vmem((tokens, channels), BF16),
        "glu": vmem((tokens + 2 * PAD, own_channels), F32),
        "gp": vmem((edge, mlp_cols[0][1]), F32),
        "up": vmem((edge, mlp_cols[0][1]), F32),
        "hidden": vmem((tokens, hidden), BF16),
        "wv": vmem((width, own_channels), BF16),
        "wg": vmem((width, own_channels), BF16),
        "wm": vmem((channels, cols), BF16),
        "wgate": vmem((width, hidden), BF16),
        "wup": vmem((width, hidden), BF16),
        "wd": vmem((shards,) + a["down"].shape, BF16),
        "early": vmem((shards - 1, tokens, LANES), F32),
        "kept": vmem((2, tokens, LANES), F32),
        "stage": vmem((blocks, tokens, LANES), BF16),
        "sib_in": vmem((blocks // CORES, tokens, LANES), BF16),
        "own_in": vmem((chips - 1, own_blocks, tokens, LANES), BF16),
        "total": vmem((own_blocks, tokens, LANES), F32),
        "stats": vmem((tps, 8, tokens), F32),
        "result": vmem((tokens, cols), BF16),
        "out_sem": dma((1,)),
        "local_sem": dma((7 + len(SMALL),)),
        "z_recv": dma((chunks, shards)),
        "up_send": dma((8,)),
        "down_send": dma((8,)),
        "y_send": dma((groups - 1, 8)),
        "y_recv": dma((groups - 1, chunks - down_blocks - 1)),
        "y_down": dma((groups - 1, down_blocks, shards)),
        "gather_send": dma((3,)),
        "gather_chip": dma((3, chips - 1, pieces)),
        "gather_core": dma((3, pieces)),
        "stage_send": dma((1,)),
        "sib_recv": dma((blocks // CORES, tokens // block_rows)),
        "own_recv": dma((chips - 1, own_blocks, tokens // block_rows)),
        "stats_send": dma((1,)),
        "stats_recv": dma((1,)),
    }
    for name in SMALL:
        scratch["v_" + name] = vmem(a[name].shape, F32)
    n = SimpleNamespace(
        inputs=INPUTS,
        small=SMALL,
        scratch=tuple(scratch),
        tps=tps,
        shards=shards,
        groups=groups,
        chips=chips,
        tokens=tokens,
        rows=rows,
        pieces=pieces,
        block_rows=block_rows,
        cols=cols,
        width=width,
        channels=channels,
        own_channels=own_channels,
        depth=depth,
        mix_depth=a["mix"].shape[0],
        hidden=hidden,
        mlp_cols=mlp_cols,
        down_blocks=down_blocks,
        whole_rows=whole_rows,
        mlp_lag=MLP_LAG,
        down_lag=DOWN_LAG,
        chunks=chunks,
        taps=a["conv_taps"].shape[0],
    )
    return pl.pallas_call(
        functools.partial(layer_kernel, n),
        out_shape=jax.ShapeDtypeStruct((tokens, cols), BF16),
        in_specs=[pl.BlockSpec(memory_space=pl.ANY)] * len(INPUTS),
        out_specs=pl.BlockSpec(memory_space=pl.ANY),
        scratch_shapes=list(scratch.values()),
        compiler_params=pltpu.CompilerParams(
            collective_id=0, has_side_effects=True, vmem_limit_bytes=GRANT
        ),
        name="layer",
    )(*[a[name] for name in INPUTS])


def solution(mesh):
    return jax.shard_map(
        local,
        mesh=mesh,
        in_specs=(
            P(("grp", "fs"), "tp"),
            P(),
            P("fs", "tp"),
            P("fs", "tp"),
            P(None, "tp"),
            P(),
            P(),
            P("fs", "tp"),
            P(),
            P("fs", "tp"),
            P("fs", "tp"),
            P(None, "tp"),
            P(None, "tp"),
            P("tp", "fs"),
            P("tp"),
        ),
        out_specs=P(("grp", "fs"), "tp"),
        check_vma=False,
    )
```
